512 devices in a mesh: grp: 2 (over y), dp: 8 (over x), kv: 16 (over z), tp: 2 (over core).
Axes of the slice: x: 8, y: 2, z: 16, core: 2. Of those that a mesh axis runs over, the one named last changes fastest.
The devices are a block of a 8x8x16 slice.
Arguments:
- queries: bfloat16 [16, 4096, 2048], P(('grp', 'dp'), 'kv', 'tp'), parts along dimension 0, may hold values from -10 to 10
- keys: bfloat16 [16, 4096, 512], P(('grp', 'dp'), 'kv', 'tp'), parts along dimension 0, may hold values from -10 to 10
- values: bfloat16 [16, 4096, 512], P(('grp', 'dp'), 'kv', 'tp'), parts along dimension 0, may hold values from -6 to 6
- gate_logits: float32 [16, 2, 4096, 32], P(('grp', 'dp'), None, 'kv', 'tp'), parts along dimension 0, may hold values from -6 to 6
- chosen: int32 [16, 32, 8, 16], P(('grp', 'dp'), 'kv', 'tp'), parts along dimension 0, may hold values from -1 to 63, as said below
- pool_k: float32 [32, 64], replicated, may hold values from 0 to 0.35
- pool_v: float32 [32, 64], replicated, may hold values from 0 to 0.35
- out_gain: float32 [2048], P('tp'), may hold values from 0.1 to 1.9
Outputs:
- attended: bfloat16 [16, 4096, 2048], P(('grp', 'dp'), 'kv', 'tp'), parts along dimension 0
The draws below stay inside these ranges and needn't reach their ends.
There are 2 independent parts, one for each index of `grp`. The reference program is written for one: setup_inputs(seed, part) draws one part's arguments, and reference() takes and returns one part's arrays. A program takes and returns all parts, laid end to end along the dimension named above; an argument that names none is the same for every part. Nothing has to cross between parts.
Inputs may be any that keep to these rules, and one draw needn't show every extreme that they name: Entries are key block numbers (block e holds positions e * 64 to e * 64 + 63) or -1 for none. The list of query block b (positions b * 128 onward) holds the blocks that contain its own positions, other distinct blocks that begin before it, and -1 in its remaining entries. For the query blocks of one span of 256 positions and one key head, the blocks chosen from any other span number at most 2; in every draw some span reaches 2.
All inputs are finite; a program needn't handle non-finite values.
Results may differ from the reference program's by a relative error of at most 0.0079.
Values may be sent and summed in bfloat16 or wider, within the bound.
No kernel may reach another device: no remote copies, remote signals or barrier semaphores. Data moves between devices by JAX's collectives and lax.ppermute only.
A program may use at most 64 MiB of HBM per device.

```python
import jax
import jax.numpy as jnp
from jax import lax

H = 32
G = 8
DH = 64
HPG = 4
CMP_STRIDE = 16
CMP_BLOCK = 32
SLC = 64
QB = 128
NSEL = 16
MOST = 2
TOK_DEV = 256
SEQS = 8
SEQLEN = 4096
N_KV = 16


def base_field(key, shape):
    return jnp.clip(jax.random.normal(key, shape, jnp.float32), -6.0, 6.0)


def draw_queries(key, part):
    field = base_field(jax.random.fold_in(key, 1), (SEQS, SEQLEN, H * DH))
    return field.astype(jnp.bfloat16)


def draw_keys(key, part):
    field = base_field(jax.random.fold_in(key, 2), (SEQS, SEQLEN, G * DH))
    return field.astype(jnp.bfloat16)


def draw_chosen(key, part):
    nqb = SEQLEN // QB
    per_owner = TOK_DEV // SLC
    total = SEQLEN // SLC
    own = QB // SLC
    per_span = TOK_DEV // QB
    base = jax.random.fold_in(key, 101)
    pop_key, set_key, pick_key = jax.random.split(base, 3)
    favour = jax.random.randint(pop_key, (SEQS, total), 0, 3)
    raw = jax.random.randint(set_key, (SEQS, N_KV, G, N_KV, per_owner), 0, 65536)
    setscore = (raw - favour.reshape(SEQS, 1, 1, N_KV, per_owner) * 40000) * per_owner + jnp.arange(per_owner)
    rank = jnp.sum(setscore[..., None, :] < setscore[..., :, None], axis=-1)
    inset = rank < MOST
    blocks = jnp.arange(nqb)
    span = blocks // per_span
    inset_q = inset[:, span].reshape(SEQS, nqb, G, total)
    number = jnp.arange(total)
    owner = number // per_owner
    remote = owner[None, :] < span[:, None]
    earlier = (owner[None, :] == span[:, None]) & (number[None, :] < blocks[:, None] * own)
    mine = number[None, :] // own == blocks[:, None]
    near = (owner[None, :] == span[:, None] - 1) | (owner[None, :] == span[:, None] - N_KV // 2) & (span[:, None] >= N_KV // 2)
    avail = remote[None, :, None, :] & inset_q | earlier[None, :, None, :]
    forced = mine[None, :, None, :] | (remote & near)[None, :, None, :] & inset_q
    noise = jax.random.randint(pick_key, (SEQS, nqb, G, total), 0, 65536) - favour[:, None, None, :] * 20000
    prio = jnp.where(forced, 0, jnp.where(avail, noise + 40001, 1 << 22))
    order = jnp.argsort(prio * total + number, axis=-1)[..., :NSEL]
    picked = jnp.take_along_axis(prio, order, axis=-1)
    return jnp.where(picked < 1 << 22, order, -1).astype(jnp.int32)


def levels(stream_key, dims, shards, smallest, largest):
    gain = 1.0
    for position, blocks in shards:
        draws = jax.random.uniform(jax.random.fold_in(jax.random.fold_in(stream_key, 6), position), (blocks,), jnp.float32, smallest / len(shards), largest / len(shards))
        gain = gain * jnp.repeat(jnp.exp(draws), dims[position] // blocks).reshape((-1,) + (1,) * (len(dims) - 1 - position))
    return gain


def normal_values(own_key, shape, deviation, most, cuts=(), held_as=jnp.bfloat16):
    result = deviation * jax.random.normal(own_key, shape, jnp.float32)
    if cuts:
        result = result * levels(own_key, shape, cuts, -0.22, 0.18)
    return jnp.clip(result, -most, most).astype(held_as)


def setup_inputs(seed: int = 0, part: int = 0) -> dict:
    streams_of = jax.random.split(jax.random.key(seed), 9)
    own_keys = jax.random.split(jax.random.fold_in(streams_of[8], part), 9)
    return {
        "queries": draw_queries(jax.random.fold_in(jax.random.fold_in(streams_of[8], part), 71), part),
        "keys": draw_keys(jax.random.fold_in(jax.random.fold_in(streams_of[8], part), 71), part),
        "values": normal_values(own_keys[2], (SEQS, SEQLEN, G * DH), 1.0, 6.0, ((0, 8), (1, 16), (2, 2))),
        "gate_logits": normal_values(own_keys[3], (SEQS, 2, SEQLEN, H), 1.5, 6.0, ((0, 8), (2, 16), (3, 2)), jnp.float32),
        "chosen": draw_chosen(jax.random.fold_in(jax.random.fold_in(streams_of[8], part), 71), part),
        "pool_k": jnp.clip(jax.random.uniform(streams_of[5], (CMP_BLOCK, DH), jnp.float32, 0.0, 0.35), 0.0, 0.35),
        "pool_v": jnp.clip(jax.random.uniform(streams_of[6], (CMP_BLOCK, DH), jnp.float32, 0.0, 0.35), 0.0, 0.35),
        "out_gain": jnp.clip(1.0 + 0.18 * jax.random.normal(streams_of[7], (H * DH,), jnp.float32), 0.1, 1.9),
    }


THETA = 500000.0
EPS = 1e-06
NEG = -1e+30

def rotate(matrix, start, heads):
    length = matrix.shape[0]
    half = DH // 2
    place = (start + jnp.arange(length)).astype(jnp.float32)
    freq = jnp.power(jnp.float32(THETA), -(2.0 * jnp.arange(half).astype(jnp.float32)) / DH)
    angle = place[:, None] * freq[None, :]
    cosine = jnp.cos(angle)[:, None, :]
    sine = jnp.sin(angle)[:, None, :]
    parts = matrix.reshape(length, heads, DH).astype(jnp.float32)
    first = parts[..., :half]
    second = parts[..., half:]
    turned = jnp.concatenate([first * cosine - second * sine, second * cosine + first * sine], -1)
    return turned.reshape(length, heads * DH).astype(jnp.bfloat16)

def compress(extended, pool, groups):
    count = extended.shape[0] // CMP_STRIDE - 1
    parts = extended.reshape(count + 1, CMP_STRIDE, groups, DH).astype(jnp.float32)
    lower = jnp.einsum('nigd,id->ngd', parts[:-1], pool[:CMP_STRIDE], precision=lax.Precision.HIGHEST)
    upper = jnp.einsum('nigd,id->ngd', parts[1:], pool[CMP_STRIDE:], precision=lax.Precision.HIGHEST)
    return (lower + upper).astype(jnp.bfloat16)

def reference(queries, keys, values, gate_logits, chosen, pool_k, pool_v, out_gain):
    scale = DH ** (-0.5)

    def one_sequence(item):
        query_seq, key_seq, value_seq, logits, lists = item
        length = query_seq.shape[0]
        query_turned = rotate(query_seq, 0, H)
        key_turned = rotate(key_seq, 0, G)
        padding = jnp.zeros((CMP_STRIDE, G * DH), key_seq.dtype)
        key_summary = compress(jnp.concatenate([key_seq, padding], 0), pool_k, G).astype(jnp.float32)
        value_summary = compress(jnp.concatenate([value_seq, padding], 0), pool_v, G).astype(jnp.float32)
        count = length // CMP_STRIDE
        ends = jnp.arange(count) * CMP_STRIDE + CMP_BLOCK - 1
        key_blocks = key_turned.reshape(length // SLC, SLC, G, DH)
        value_blocks = value_seq.reshape(length // SLC, SLC, G, DH)
        group_pick = jnp.arange(G)[:, None]

        def block(index):
            start = index * QB
            place = start + jnp.arange(QB)
            query_rows = lax.dynamic_slice_in_dim(query_seq, start, QB, 0).reshape(QB, G, HPG, DH).astype(jnp.float32)
            query_turn = lax.dynamic_slice_in_dim(query_turned, start, QB, 0).reshape(QB, G, HPG, DH).astype(jnp.float32)
            score = jnp.einsum('tghd,ngd->ghtn', query_rows, key_summary) * scale
            allow = (ends[None, :] <= place[:, None])[None, None]
            score = jnp.where(allow, score, NEG)
            top = lax.optimization_barrier(jnp.max(score, -1, keepdims=True))
            weight = jnp.where(allow, jnp.exp(score - top), 0.0)
            total = jnp.maximum(lax.optimization_barrier(jnp.sum(weight, -1)), 1.0)
            rounded = lax.optimization_barrier(weight.astype(jnp.bfloat16)).astype(jnp.float32)
            summary_out = jnp.einsum('ghtn,ngd->ghtd', rounded, value_summary) / total[..., None]
            picks = lists[index]
            safe = jnp.maximum(picks, 0)
            key_sel = key_blocks[safe, :, group_pick, :].astype(jnp.float32)
            value_sel = value_blocks[safe, :, group_pick, :].reshape(G, NSEL * SLC, DH).astype(jnp.float32)
            key_place = (safe[..., None] * SLC + jnp.arange(SLC)).reshape(G, NSEL * SLC)
            live = jnp.broadcast_to(picks[..., None] >= 0, (G, NSEL, SLC)).reshape(G, NSEL * SLC)
            allow_sel = (live[:, None, :] & (key_place[:, None, :] <= place[None, :, None]))[:, None]
            chosen_score = jnp.einsum('tghd,gnkd->ghtnk', query_turn, key_sel).reshape(G, HPG, QB, NSEL * SLC) * scale
            chosen_score = jnp.where(allow_sel, chosen_score, NEG)
            top_sel = lax.optimization_barrier(jnp.max(chosen_score, -1, keepdims=True))
            weight_sel = jnp.where(allow_sel, jnp.exp(chosen_score - top_sel), 0.0)
            total_sel = lax.optimization_barrier(jnp.sum(weight_sel, -1))
            rounded_sel = lax.optimization_barrier(weight_sel.astype(jnp.bfloat16)).astype(jnp.float32)
            chosen_out = jnp.einsum('ghtk,gkd->ghtd', rounded_sel, value_sel) / total_sel[..., None]
            gates = jax.nn.sigmoid(lax.dynamic_slice_in_dim(logits, start, QB, 1))
            gates = gates.reshape(2, QB, G, HPG).transpose(0, 2, 3, 1)
            mixed = gates[0][..., None] * summary_out + gates[1][..., None] * chosen_out
            mixed = mixed.transpose(2, 0, 1, 3).reshape(QB, H, DH)
            normed = mixed * lax.rsqrt(lax.optimization_barrier(jnp.mean(mixed * mixed, -1, keepdims=True)) + EPS) * out_gain.reshape(H, DH)
            return normed.reshape(QB, H * DH).astype(jnp.bfloat16)
        return lax.map(block, jnp.arange(length // QB)).reshape(length, H * DH)
    return lax.map(one_sequence, (queries, keys, values, gate_logits, chosen))
```

```python
import functools
import math

import jax
import jax.numpy as jnp
import numpy as np
from jax import lax
from jax.experimental import pallas as pl
from jax.experimental.pallas import tpu as pltpu
from jax.sharding import PartitionSpec as P

DH = 64
CMP_STRIDE = 16
CMP_BLOCK = 32
SLC = 64
QB = 128
NSEL = 16
THETA = 500000.0
EPS = 1e-06
NEG = -1e30
SCALE2 = DH ** (-0.5) * math.log2(math.e)
LANES = 128
F32 = jnp.float32
BF16 = jnp.bfloat16


def lane_of(rows):
    return lax.broadcasted_iota(jnp.int32, (rows, LANES), 1)


def swap_halves(x, lane):
    return jnp.where(lane % DH < DH // 2, pltpu.roll(x, 96, 1), pltpu.roll(x, 32, 1))


def trig(span, cosa, sina, cosb, sinb):
    ca = cosa[pl.ds(span, 1), :]
    sa = sina[pl.ds(span, 1), :]
    cos = ca * cosb - sa * sinb
    sin = sa * cosb + ca * sinb
    lane = lane_of(cosb.shape[0])
    return cos, jnp.where(lane % DH < DH // 2, -sin, sin)


def dot_t(a, b):
    return lax.dot_general(a, b, (((1,), (1,)), ((), ())), preferred_element_type=F32)


def dot_n(a, b):
    return lax.dot_general(a, b, (((1,), (0,)), ((), ())), preferred_element_type=F32)


def keep_half(x, odd):
    lane = lane_of(x.shape[0])
    return jnp.where((lane >= DH) if odd else (lane < DH), x, 0.0)


def with_ones(x, odd):
    ones = keep_half(jnp.ones((x.shape[0], LANES), F32), odd)
    return jnp.concatenate([keep_half(x, odd), ones], 1).astype(BF16)


def pools(piece, pool_ref, lu_ref, i):
    x = piece.astype(F32).reshape(16, CMP_STRIDE, -1)
    lower = jnp.sum(x * pool_ref[0:CMP_STRIDE, :][None], 1)
    upper = jnp.sum(x * pool_ref[CMP_STRIDE:CMP_BLOCK, :][None], 1)
    lu_ref[i, 0] = lower
    lu_ref[i, 1] = upper


def online(qrot_ref, rk, rv, bias_of, acc_in, m_in, acc_ref, m_ref, p):
    for b in range(2):
        s = dot_t(qrot_ref[p, b], rk) * SCALE2
        s = bias_of(b, s)
        n = s.shape[1] // LANES
        me = functools.reduce(jnp.maximum, [s[:, i * LANES:(i + 1) * LANES] for i in range(n) if bias_of.odd[i] == 0])
        mo = functools.reduce(jnp.maximum, [s[:, i * LANES:(i + 1) * LANES] for i in range(n) if bias_of.odd[i] == 1])
        rows = s.shape[0]
        me = jnp.broadcast_to(jnp.max(me, 1, keepdims=True), (rows, LANES))
        mo = jnp.broadcast_to(jnp.max(mo, 1, keepdims=True), (rows, LANES))
        if acc_in is not None:
            olde = m_in[p, b, 0]
            oldo = m_in[p, b, 1]
            me = jnp.maximum(me, olde)
            mo = jnp.maximum(mo, oldo)
            alpha = jnp.exp2(jnp.where(lane_of(rows) < DH, olde - me, oldo - mo))
        m_ref[p, b, 0] = me
        m_ref[p, b, 1] = mo
        w = jnp.concatenate(
            [jnp.exp2(s[:, i * LANES:(i + 1) * LANES] - (mo if bias_of.odd[i] else me)).astype(BF16) for i in range(n)], 1
        )
        out = dot_n(w, rv)
        if acc_in is not None:
            out = acc_in[p, b] * jnp.concatenate([alpha, alpha], 1) + out
        acc_ref[p, b] = out


class Bias:
    def __init__(self, odd, fn):
        self.odd = odd
        self.fn = fn

    def __call__(self, b, s):
        return self.fn(b, s)


def prep_body(tab, q_ref, k_ref, v_ref, lg_ref, pool_ref, cosa, sina, cosb_ref, sinb_ref,
              qrot_ref, qraw_ref, gates_ref, acc_ref, m_ref, lu_ref):
    my = tab[0]
    length = q_ref.shape[0]
    cos, sin = trig(my, cosa, sina, cosb_ref[...], sinb_ref[...])
    lane = lane_of(length)
    lg = jax.nn.sigmoid(lg_ref[0]), jax.nn.sigmoid(lg_ref[1])
    for p in range(2):
        for j in range(4):
            tiles = []
            for odd in range(2):
                t = 4 * p + 2 * odd + j // 2
                x = q_ref[:, t * LANES:(t + 1) * LANES].astype(F32)
                turned = x * cos + swap_halves(x, lane) * sin
                if (j % 2) != odd:
                    x = pltpu.roll(x, DH, 1)
                    turned = pltpu.roll(turned, DH, 1)
                tiles.append((x, turned))
            raw = jnp.where(lane < DH, tiles[0][0], tiles[1][0]).astype(BF16)
            rot = jnp.where(lane < DH, tiles[0][1], tiles[1][1]).astype(BF16)
            he, ho = 8 * p + j, 8 * p + 4 + j
            gs = [jnp.where(lane < DH, lg[i][:, he:he + 1], lg[i][:, ho:ho + 1]) for i in range(2)]
            for b in range(2):
                rows = slice(b * QB, (b + 1) * QB)
                dst = slice(j * QB, (j + 1) * QB)
                qraw_ref[p, b, dst, :] = raw[rows]
                qrot_ref[p, b, dst, :] = rot[rows]
                gates_ref[0, p, b, dst, :] = gs[0][rows]
                gates_ref[1, p, b, dst, :] = gs[1][rows]
    both = jnp.concatenate([k_ref[...], v_ref[...]], 1)
    pools(both, pool_ref, lu_ref, 0)
    key_pos = lax.broadcasted_iota(jnp.int32, (QB, length), 1)
    row_pos = lax.broadcasted_iota(jnp.int32, (QB, length), 0)
    blk = lax.broadcasted_iota(jnp.int32, (1, length), 1) // SLC
    for p in range(2):
        kx = k_ref[:, p * LANES:(p + 1) * LANES].astype(F32)
        kx = kx * cos + swap_halves(kx, lane) * sin
        vx = v_ref[:, p * LANES:(p + 1) * LANES].astype(F32)
        rk = jnp.concatenate([keep_half(kx, 0), keep_half(kx, 1)], 0).astype(BF16)
        rv = jnp.concatenate([with_ones(vx, 0), with_ones(vx, 1)], 0)

        def own_bias(b, s, p=p):
            cols = []
            for odd in range(2):
                row = jnp.zeros((1, length), jnp.int32)
                for i in range(4):
                    row = jnp.where(blk == i, tab[1 + (b * 4 + 2 * p + odd) * 4 + i], row)
                ok = (row > 0) & (key_pos <= row_pos + b * QB)
                cols.append(jnp.where(ok, 0.0, NEG))
            bias = jnp.concatenate(cols, 1)
            return s + jnp.concatenate([bias] * 4, 0)

        online(qrot_ref, rk, rv, Bias([0, 0, 1, 1], own_bias), None, None, acc_ref, m_ref, p)


OWN = 1 + 2 * 4 * 4


def step_body(spans, pieces, tab, pool_ref, cosa, sina, cosb_ref, sinb_ref, qrot_ref, acc_in, m_in, acc_ref, m_ref, lu_ref, rk_ref, rv_ref):
    for i, piece in enumerate(pieces):
        pools(piece[...], pool_ref, lu_ref, i)
    lane = lane_of(SLC)
    col = lax.broadcasted_iota(jnp.int32, (1, LANES), 1)
    for p in range(2):
        for i, (piece, span) in enumerate(zip(pieces, spans)):
            for odd in range(2):
                for slot in range(2):
                    base = OWN + (span * 4 + 2 * p + odd) * 6
                    at = pl.multiple_of(tab[base + slot] * SLC, SLC)
                    cos, sin = trig(span, cosa, sina, cosb_ref[pl.ds(at, SLC), :], sinb_ref[pl.ds(at, SLC), :])
                    kx = piece[pl.ds(at, SLC), p * LANES:(p + 1) * LANES].astype(F32)
                    kx = kx * cos + swap_halves(kx, lane) * sin
                    vx = piece[pl.ds(at, SLC), (2 + p) * LANES:(3 + p) * LANES].astype(F32)
                    dst = slice(i * 256 + odd * 128 + slot * 64, i * 256 + odd * 128 + slot * 64 + 64)
                    rk_ref[p, dst, :] = keep_half(kx, odd).astype(BF16)
                    rv_ref[p, dst, :] = with_ones(vx, odd)

        def bias(b, s, p=p):
            cols = []
            for span in spans:
                for odd in range(2):
                    base = OWN + (span * 4 + 2 * p + odd) * 6 + 2 + b * 2
                    row = jnp.where(col < SLC, tab[base], tab[base + 1])
                    cols.append(jnp.where(row > 0, 0.0, NEG))
            return s + jnp.concatenate(cols, 1)

        online(qrot_ref, rk_ref[p], rv_ref[p], Bias([0, 1] * len(pieces), bias), acc_in, m_in, acc_ref, m_ref, p)


def pair_kernel(k, n, tab, pf_ref, pb_ref, pool_ref, cosa, sina, cosb_ref, sinb_ref, qrot_ref, acc_in, m_in,
                acc_ref, m_ref, lu_ref, rk_ref, rv_ref):
    my = tab[0]
    spans = [lax.rem(my + n - k, n), lax.rem(my + k, n)]
    step_body(spans, [pf_ref, pb_ref], tab, pool_ref, cosa, sina, cosb_ref, sinb_ref, qrot_ref, acc_in, m_in, acc_ref, m_ref, lu_ref, rk_ref, rv_ref)


def final_kernel(k, n, tab, pf_ref, pb_ref, pool_ref, cosa, sina, cosb_ref, sinb_ref, qrot_ref, acc_in, m_in,
                 qraw_ref, gates_ref, gain_ref, *rest):
    parts, (out_ref, acc_ref, m_ref, lu_ref, rk_ref, rv_ref, piece_ref, last_ref) = rest[:k], rest[k:]
    my = tab[0]
    half = pf_ref.shape[0]
    piece_ref[:half, :] = pf_ref[...]
    piece_ref[half:, :] = pb_ref[...]
    step_body([lax.rem(my + n - k, n)], [piece_ref], tab, pool_ref, cosa, sina, cosb_ref, sinb_ref, qrot_ref, acc_in, m_in, acc_ref, m_ref, last_ref, rk_ref, rv_ref)
    lu_ref[:, 16 * n:, :] = jnp.zeros((2, 16, lu_ref.shape[2]), F32)

    def place(part, i, span):
        at = pl.multiple_of(span * 16, 16)
        for half in range(2):
            lu_ref[half, pl.ds(at, 16), :] = part[i, half]

    place(parts[0], 0, my)
    for d in range(1, k):
        place(parts[d], 0, lax.rem(my + n - d, n))
        place(parts[d], 1, lax.rem(my + d, n))
    place(last_ref, 0, lax.rem(my + n - k, n))
    count = 16 * n
    sums = (lu_ref[0, 0:count, :] + lu_ref[1, 1:count + 1, :]).astype(BF16).astype(F32)
    length = 2 * QB
    ends = lax.broadcasted_iota(jnp.int32, (QB, count), 1) * CMP_STRIDE + CMP_BLOCK - 1
    row_pos = lax.broadcasted_iota(jnp.int32, (QB, count), 0)
    rows = 4 * QB
    lane = lane_of(rows)
    lane1 = lane_of(QB)
    sq = lax.broadcasted_iota(jnp.int32, (LANES, LANES), 0) // DH == lax.broadcasted_iota(jnp.int32, (LANES, LANES), 1) // DH
    sq = jnp.where(sq, 1.0 / DH, 0.0).astype(BF16)
    for p in range(2):
        ks = sums[:, p * LANES:(p + 1) * LANES]
        vs = sums[:, (2 + p) * LANES:(3 + p) * LANES]
        for b in range(2):
            ok = ends <= row_pos + (my * length + b * QB)
            ok = jnp.concatenate([ok] * 4, 0)
            out = None
            for odd in range(2):
                s = dot_t(qraw_ref[p, b], keep_half(ks, odd).astype(BF16)) * SCALE2
                s = jnp.where(ok, s, NEG)
                top = jnp.max(s, 1, keepdims=True)
                w = jnp.where(ok, jnp.exp2(s - top), 0.0).astype(BF16)
                o = dot_n(w, with_ones(vs, odd))
                out = o if out is None else out + o
            summary = out[:, :LANES] / jnp.maximum(out[:, LANES:], 1.0)
            acc = acc_ref[p, b]
            chosen = acc[:, :LANES] / acc[:, LANES:]
            mixed = gates_ref[0, p, b] * summary + gates_ref[1, p, b] * chosen
            m2 = mixed * mixed
            hi = m2.astype(BF16)
            lo = (m2 - hi.astype(F32)).astype(BF16)
            mean = dot_n(hi, sq) + dot_n(lo, sq)
            r = mixed * lax.rsqrt(mean + EPS)
            for tt in range(4):
                j0 = (tt % 2) * 2
                x = r[j0 * QB:(j0 + 1) * QB]
                y = r[(j0 + 1) * QB:(j0 + 2) * QB]
                if tt < 2:
                    z = jnp.where(lane1 < DH, x, pltpu.roll(y, DH, 1))
                else:
                    z = jnp.where(lane1 < DH, pltpu.roll(x, DH, 1), y)
                t = 4 * p + tt
                z = z * gain_ref[:, t * LANES:(t + 1) * LANES]
                out_ref[b * QB:(b + 1) * QB, t * LANES:(t + 1) * LANES] = z.astype(BF16)


def table_of(lists, my, n):
    groups = lists.shape[1]
    per = 256 // SLC
    sel = jnp.any(lists[:, :, None, :] == jnp.arange(n * per)[None, None, :, None], -1)
    sel = sel.reshape(2, groups, n, per).transpose(0, 2, 1, 3)
    own = lax.dynamic_slice_in_dim(sel, my, 1, 1)[:, 0].astype(jnp.int32)
    union = sel[0] | sel[1]
    u = union.astype(jnp.int32)
    before = jnp.stack([sum((u[..., i] for i in range(j)), jnp.zeros_like(u[..., 0])) for j in range(per)], -1)
    cols = []
    hits = [union & (before == slot) for slot in range(2)]
    for slot in range(2):
        cols.append(jnp.sum(jnp.where(hits[slot], jnp.arange(per), 0), -1))
    for b in range(2):
        for slot in range(2):
            cols.append(jnp.any(hits[slot] & sel[b], -1).astype(jnp.int32))
    tab = jnp.stack(cols, -1).reshape(-1)
    return jnp.concatenate([my.reshape(1).astype(jnp.int32), own.reshape(-1), tab.astype(jnp.int32)])


VM = pl.BlockSpec(memory_space=pltpu.VMEM)
SM = pl.BlockSpec(memory_space=pltpu.SMEM)


def per_device(n, queries, keys, values, gate_logits, chosen, pool_k, pool_v, out_gain):
    queries, keys, values = queries[0], keys[0], values[0]
    logits, lists = gate_logits[0], chosen[0]
    length = queries.shape[0]
    groups = keys.shape[1] // DH
    my = lax.axis_index("kv")
    fw = [(i, (i + 1) % n) for i in range(n)]
    bw = [((i + 1) % n, i) for i in range(n)]
    piece = jnp.concatenate([keys, values], 1)
    half = length // 2

    def hop(x, route):
        return lax.ppermute(x, "kv", route)

    f, g = hop(piece, fw), hop(piece, bw)

    freq = THETA ** (-2.0 * np.arange(DH // 2) / DH)
    freq = np.tile(freq, LANES // (DH // 2))
    ang_a = (np.arange(n) * length)[:, None] * freq[None, :]
    ang_b = np.arange(length)[:, None] * freq[None, :]
    trigs = [jnp.asarray(a, F32) for a in (np.cos(ang_a), np.sin(ang_a), np.cos(ang_b), np.sin(ang_b))]
    pool = jnp.concatenate([jnp.tile(pool_k, (1, groups)), jnp.tile(pool_v, (1, groups))], 1)
    tab = table_of(lists, my, n)
    rows = 4 * QB
    count = n * 16
    qs = jax.ShapeDtypeStruct((2, 2, rows, LANES), BF16)
    accs = jax.ShapeDtypeStruct((2, 2, rows, 2 * LANES), F32)
    ms = jax.ShapeDtypeStruct((2, 2, 2, rows, LANES), F32)
    def lus(pieces):
        return jax.ShapeDtypeStruct((pieces, 2, 16, 2 * keys.shape[1]), F32)

    gs = jax.ShapeDtypeStruct((2, 2, 2, rows, LANES), F32)
    cost = pl.CostEstimate(flops=2_000_000_000, bytes_accessed=4_000_000, transcendentals=1_000_000)
    params = pltpu.CompilerParams(vmem_limit_bytes=48 * 1024 * 1024)
    qrot, qraw, gates, acc, m, lu = pl.pallas_call(
        prep_body, out_shape=(qs, qs, gs, accs, ms, lus(1)),
        in_specs=[SM] + [VM] * 9, out_specs=(VM,) * 6, compiler_params=params, cost_estimate=cost, name="prep",
    )(tab, queries, keys, values, logits, pool, *trigs)

    parts = [lu]
    for k in range(1, 9):
        if k < 7:
            f2, g2 = hop(f, fw), hop(g, bw)
        elif k == 7:
            f2, g2 = hop(f[:half], fw), hop(g[half:], bw)
        if k < 8:
            acc, m, lu = pl.pallas_call(
                functools.partial(pair_kernel, k, n), out_shape=(accs, ms, lus(2)),
                in_specs=[SM] + [VM] * 10, out_specs=(VM,) * 3,
                input_output_aliases={9: 0, 10: 1},
                scratch_shapes=[pltpu.VMEM((2, 512, LANES), BF16), pltpu.VMEM((2, 512, 2 * LANES), BF16)],
                compiler_params=params, cost_estimate=cost, name=f"pair{k}",
            )(tab, f, g, pool, *trigs, qrot, acc, m)
            parts.append(lu)
            f, g = f2, g2
        else:
            out = pl.pallas_call(
                functools.partial(final_kernel, k, n),
                out_shape=jax.ShapeDtypeStruct(queries.shape, BF16),
                in_specs=[SM] + [VM] * (13 + len(parts)), out_specs=VM,
                scratch_shapes=[pltpu.VMEM(accs.shape, F32), pltpu.VMEM(ms.shape, F32), pltpu.VMEM((2, count + 16, 2 * keys.shape[1]), F32),
                                pltpu.VMEM((2, 256, LANES), BF16), pltpu.VMEM((2, 256, 2 * LANES), BF16),
                                pltpu.VMEM((length, 2 * keys.shape[1]), BF16), pltpu.VMEM(lus(1).shape, F32)],
                compiler_params=params, cost_estimate=cost, name="final",
            )(tab, f, g, pool, *trigs, qrot, acc, m, qraw, gates, out_gain.reshape(1, -1), *parts)
    return out[None]


def solution(mesh):
    in_specs = (
        P(("grp", "dp"), "kv", "tp"),
        P(("grp", "dp"), "kv", "tp"),
        P(("grp", "dp"), "kv", "tp"),
        P(("grp", "dp"), None, "kv", "tp"),
        P(("grp", "dp"), "kv", "tp", None),
        P(),
        P(),
        P("tp"),
    )
    out_specs = P(("grp", "dp"), "kv", "tp")
    return jax.shard_map(
        functools.partial(per_device, mesh.shape["kv"]), mesh=mesh, in_specs=in_specs, out_specs=out_specs, check_vma=False
    )
```

```python
import functools
import math

import jax
import jax.numpy as jnp
import numpy as np
from jax import lax
from jax.experimental import pallas as pl
from jax.experimental.pallas import tpu as pltpu
from jax.sharding import PartitionSpec as P

DH = 64
CMP_STRIDE = 16
CMP_BLOCK = 32
SLC = 64
QB = 128
NSEL = 16
THETA = 500000.0
EPS = 1e-06
NEG = -1e30
SCALE2 = DH ** (-0.5) * math.log2(math.e)
LANES = 128
F32 = jnp.float32
BF16 = jnp.bfloat16


def lane_of(rows):
    return lax.broadcasted_iota(jnp.int32, (rows, LANES), 1)


def swap_halves(x, lane):
    return jnp.where(lane % DH < DH // 2, pltpu.roll(x, 96, 1), pltpu.roll(x, 32, 1))


def trig(span, cosa, sina, cosb, sinb):
    ca = cosa[pl.ds(span, 1), :]
    sa = sina[pl.ds(span, 1), :]
    cos = ca * cosb - sa * sinb
    sin = sa * cosb + ca * sinb
    lane = lane_of(cosb.shape[0])
    return cos, jnp.where(lane % DH < DH // 2, -sin, sin)


def dot_t(a, b):
    return lax.dot_general(a, b, (((1,), (1,)), ((), ())), preferred_element_type=F32)


def dot_n(a, b):
    return lax.dot_general(a, b, (((1,), (0,)), ((), ())), preferred_element_type=F32)


def keep_half(x, odd):
    lane = lane_of(x.shape[0])
    return jnp.where((lane >= DH) if odd else (lane < DH), x, 0.0)


def with_ones(x, odd):
    ones = keep_half(jnp.ones((x.shape[0], LANES), F32), odd)
    return jnp.concatenate([keep_half(x, odd), ones], 1).astype(BF16)


def pools(piece, pool_ref, lu_ref, i):
    x = piece.astype(F32).reshape(16, CMP_STRIDE, -1)
    lower = jnp.sum(x * pool_ref[0:CMP_STRIDE, :][None], 1)
    upper = jnp.sum(x * pool_ref[CMP_STRIDE:CMP_BLOCK, :][None], 1)
    lu_ref[i, 0] = lower
    lu_ref[i, 1] = upper


def online(qrot_ref, rk, rv, bias_of, acc_in, m_in, acc_ref, m_ref, p):
    for b in range(2):
        s = dot_t(qrot_ref[p, b], rk) * SCALE2
        s = bias_of(b, s)
        n = s.shape[1] // LANES
        me = functools.reduce(jnp.maximum, [s[:, i * LANES:(i + 1) * LANES] for i in range(n) if bias_of.odd[i] == 0])
        mo = functools.reduce(jnp.maximum, [s[:, i * LANES:(i + 1) * LANES] for i in range(n) if bias_of.odd[i] == 1])
        rows = s.shape[0]
        me = jnp.broadcast_to(jnp.max(me, 1, keepdims=True), (rows, LANES))
        mo = jnp.broadcast_to(jnp.max(mo, 1, keepdims=True), (rows, LANES))
        if acc_in is not None:
            olde = m_in[p, b, 0]
            oldo = m_in[p, b, 1]
            me = jnp.maximum(me, olde)
            mo = jnp.maximum(mo, oldo)
            alpha = jnp.exp2(jnp.where(lane_of(rows) < DH, olde - me, oldo - mo))
        m_ref[p, b, 0] = me
        m_ref[p, b, 1] = mo
        w = jnp.concatenate(
            [jnp.exp2(s[:, i * LANES:(i + 1) * LANES] - (mo if bias_of.odd[i] else me)).astype(BF16) for i in range(n)], 1
        )
        out = dot_n(w, rv)
        if acc_in is not None:
            out = acc_in[p, b] * jnp.concatenate([alpha, alpha], 1) + out
        acc_ref[p, b] = out


class Bias:
    def __init__(self, odd, fn):
        self.odd = odd
        self.fn = fn

    def __call__(self, b, s):
        return self.fn(b, s)


def prep_body(tab, q_hbm, k_hbm, v_hbm, lg_hbm, pk_hbm, pv_hbm, cosa_hbm, sina_hbm, cosb_hbm, sinb_hbm,
              qrot_ref, qraw_ref, gates_ref, acc_ref, m_ref, lu_ref, pool_ref, cosa, sina, cosb_ref, sinb_ref,
              q_ref, k_ref, v_ref, lg_ref, pk_ref, pv_ref, sems):
    my = tab[0]
    moves = [pltpu.make_async_copy(src, dst, sems.at[i]) for i, (src, dst) in enumerate(
        [(q_hbm, q_ref), (k_hbm, k_ref), (v_hbm, v_ref), (lg_hbm, lg_ref), (pk_hbm, pk_ref), (pv_hbm, pv_ref),
         (cosa_hbm, cosa), (sina_hbm, sina), (cosb_hbm, cosb_ref), (sinb_hbm, sinb_ref)])]
    for move in moves:
        move.start()
    for move in moves:
        move.wait()
    for i, ref in enumerate((pk_ref, pv_ref)):
        two = jnp.concatenate([ref[...], ref[...]], 1)
        pool_ref[:, 2 * i * LANES:2 * (i + 1) * LANES] = jnp.concatenate([two, two], 1)
    length = q_ref.shape[0]
    cos, sin = trig(my, cosa, sina, cosb_ref[...], sinb_ref[...])
    lane = lane_of(length)
    lg = jax.nn.sigmoid(lg_ref[0]), jax.nn.sigmoid(lg_ref[1])
    for p in range(2):
        for j in range(4):
            tiles = []
            for odd in range(2):
                t = 4 * p + 2 * odd + j // 2
                x = q_ref[:, t * LANES:(t + 1) * LANES].astype(F32)
                turned = x * cos + swap_halves(x, lane) * sin
                if (j % 2) != odd:
                    x = pltpu.roll(x, DH, 1)
                    turned = pltpu.roll(turned, DH, 1)
                tiles.append((x, turned))
            raw = jnp.where(lane < DH, tiles[0][0], tiles[1][0]).astype(BF16)
            rot = jnp.where(lane < DH, tiles[0][1], tiles[1][1]).astype(BF16)
            he, ho = 8 * p + j, 8 * p + 4 + j
            gs = [jnp.where(lane < DH, lg[i][:, he:he + 1], lg[i][:, ho:ho + 1]) for i in range(2)]
            for b in range(2):
                rows = slice(b * QB, (b + 1) * QB)
                dst = slice(j * QB, (j + 1) * QB)
                qraw_ref[p, b, dst, :] = raw[rows]
                qrot_ref[p, b, dst, :] = rot[rows]
                gates_ref[0, p, b, dst, :] = gs[0][rows]
                gates_ref[1, p, b, dst, :] = gs[1][rows]
    both = jnp.concatenate([k_ref[...], v_ref[...]], 1)
    pools(both, pool_ref, lu_ref, 0)
    key_pos = lax.broadcasted_iota(jnp.int32, (QB, length), 1)
    row_pos = lax.broadcasted_iota(jnp.int32, (QB, length), 0)
    blk = lax.broadcasted_iota(jnp.int32, (1, length), 1) // SLC
    @pl.loop(0, 2)
    def _(p):
        at = pl.multiple_of(p * LANES, LANES)
        kx = k_ref[:, pl.ds(at, LANES)].astype(F32)
        kx = kx * cos + swap_halves(kx, lane) * sin
        vx = v_ref[:, pl.ds(at, LANES)].astype(F32)
        rk = jnp.concatenate([keep_half(kx, 0), keep_half(kx, 1)], 0).astype(BF16)
        rv = jnp.concatenate([with_ones(vx, 0), with_ones(vx, 1)], 0)

        def own_bias(b, s):
            cols = []
            for odd in range(2):
                row = jnp.zeros((1, length), jnp.int32)
                for i in range(4):
                    row = jnp.where(blk == i, tab[1 + (b * 4 + 2 * p + odd) * 4 + i], row)
                ok = (row > 0) & (key_pos <= row_pos + b * QB)
                cols.append(jnp.where(ok, 0.0, NEG))
            bias = jnp.concatenate(cols, 1)
            return s + jnp.concatenate([bias] * 4, 0)

        online(qrot_ref, rk, rv, Bias([0, 0, 1, 1], own_bias), None, None, acc_ref, m_ref, p)


OWN = 1 + 2 * 4 * 4


def step_body(spans, pieces, tab, pool_ref, cosa, sina, cosb_ref, sinb_ref, qrot_ref, acc_in, m_in, acc_ref, m_ref, lu_ref, rk_ref, rv_ref):
    for i, piece in enumerate(pieces):
        pools(piece[...], pool_ref, lu_ref, i)
    lane = lane_of(SLC)
    col = lax.broadcasted_iota(jnp.int32, (1, LANES), 1)

    @pl.loop(0, 2)
    def _(p):
        kat = pl.multiple_of(p * LANES, LANES)
        vat = pl.multiple_of((2 + p) * LANES, LANES)
        for i, (piece, span) in enumerate(zip(pieces, spans)):
            for odd in range(2):
                for slot in range(2):
                    base = OWN + (span * 4 + 2 * p + odd) * 6
                    at = pl.multiple_of(tab[base + slot] * SLC, SLC)
                    cos, sin = trig(span, cosa, sina, cosb_ref[pl.ds(at, SLC), :], sinb_ref[pl.ds(at, SLC), :])
                    kx = piece[pl.ds(at, SLC), pl.ds(kat, LANES)].astype(F32)
                    kx = kx * cos + swap_halves(kx, lane) * sin
                    vx = piece[pl.ds(at, SLC), pl.ds(vat, LANES)].astype(F32)
                    dst = slice(i * 256 + odd * 128 + slot * 64, i * 256 + odd * 128 + slot * 64 + 64)
                    rk_ref[p, dst, :] = keep_half(kx, odd).astype(BF16)
                    rv_ref[p, dst, :] = with_ones(vx, odd)

        def bias(b, s):
            cols = []
            for span in spans:
                for odd in range(2):
                    base = OWN + (span * 4 + 2 * p + odd) * 6 + 2 + b * 2
                    row = jnp.where(col < SLC, tab[base], tab[base + 1])
                    cols.append(jnp.where(row > 0, 0.0, NEG))
            return s + jnp.concatenate(cols, 1)

        online(qrot_ref, rk_ref[p, 0:256 * len(pieces)], rv_ref[p, 0:256 * len(pieces)], Bias([0, 1] * len(pieces), bias), acc_in, m_in, acc_ref, m_ref, p)


def pair_kernel(n, tab, step, pf_ref, pb_ref, pool_ref, cosa, sina, cosb_ref, sinb_ref, qrot_ref, acc_in, m_in,
                acc_ref, m_ref, lu_ref, rk_ref, rv_ref):
    my = tab[0]
    k = step[0]
    ahead = my - k
    behind = my + k - n
    both = behind >= 0
    one = (ahead >= 0) & (behind < 0)

    @pl.when(both)
    def _():
        step_body([ahead, behind], [pf_ref, pb_ref], tab, pool_ref, cosa, sina, cosb_ref, sinb_ref, qrot_ref,
                  acc_in, m_in, acc_ref, m_ref, lu_ref, rk_ref, rv_ref)

    @pl.when(one)
    def _():
        step_body([ahead], [pf_ref], tab, pool_ref, cosa, sina, cosb_ref, sinb_ref, qrot_ref,
                  acc_in, m_in, acc_ref, m_ref, lu_ref, rk_ref, rv_ref)
        lu_ref[1] = jnp.zeros(lu_ref.shape[1:], F32)

    @pl.when(ahead < 0)
    def _():
        acc_ref[...] = acc_in[...]
        m_ref[...] = m_in[...]
        lu_ref[...] = jnp.zeros(lu_ref.shape, F32)


def final_kernel(k, n, tab, pf_ref, pb_ref, pool_ref, cosa, sina, cosb_ref, sinb_ref, qrot_ref, acc_in, m_in,
                 qraw_ref, gates_ref, gain_ref, *rest):
    parts, (out_ref, acc_ref, m_ref, lu_ref, rk_ref, rv_ref, piece_ref, last_ref) = rest[:k], rest[k:]
    my = tab[0]
    half = pf_ref.shape[0]

    @pl.when(my >= k)
    def _():
        piece_ref[:half, :] = pf_ref[...]
        piece_ref[half:, :] = pb_ref[...]
        step_body([my - k], [piece_ref], tab, pool_ref, cosa, sina, cosb_ref, sinb_ref, qrot_ref,
                  acc_in, m_in, acc_ref, m_ref, last_ref, rk_ref, rv_ref)

    @pl.when(my < k)
    def _():
        acc_ref[...] = acc_in[...]
        last_ref[...] = jnp.zeros(last_ref.shape, F32)

    lu_ref[:, 16 * n:, :] = jnp.zeros((2, 16, lu_ref.shape[2]), F32)

    def place(part, i, span):
        at = pl.multiple_of(span * 16, 16)
        for half in range(2):
            lu_ref[half, pl.ds(at, 16), :] = part[i, half]

    place(parts[0], 0, my)
    for d in range(1, k):
        place(parts[d], 0, lax.rem(my + n - d, n))
        place(parts[d], 1, lax.rem(my + d, n))
    place(last_ref, 0, lax.rem(my + n - k, n))
    count = 16 * n
    sums = (lu_ref[0, 0:count, :] + lu_ref[1, 1:count + 1, :]).astype(BF16).astype(F32)
    length = 2 * QB
    ends = lax.broadcasted_iota(jnp.int32, (QB, count), 1) * CMP_STRIDE + CMP_BLOCK - 1
    row_pos = lax.broadcasted_iota(jnp.int32, (QB, count), 0)
    rows = 4 * QB
    lane = lane_of(rows)
    lane1 = lane_of(QB)
    sq = lax.broadcasted_iota(jnp.int32, (LANES, LANES), 0) // DH == lax.broadcasted_iota(jnp.int32, (LANES, LANES), 1) // DH
    sq = jnp.where(sq, 1.0 / DH, 0.0).astype(BF16)
    for p in range(2):
        ks = sums[:, p * LANES:(p + 1) * LANES]
        vs = sums[:, (2 + p) * LANES:(3 + p) * LANES]
        for b in range(2):
            ok = ends <= row_pos + (my * length + b * QB)
            ok = jnp.concatenate([ok] * 4, 0)
            out = None
            for odd in range(2):
                s = dot_t(qraw_ref[p, b], keep_half(ks, odd).astype(BF16)) * SCALE2
                s = jnp.where(ok, s, NEG)
                top = jnp.max(s, 1, keepdims=True)
                w = jnp.where(ok, jnp.exp2(s - top), 0.0).astype(BF16)
                o = dot_n(w, with_ones(vs, odd))
                out = o if out is None else out + o
            summary = out[:, :LANES] / jnp.maximum(out[:, LANES:], 1.0)
            acc = acc_ref[p, b]
            chosen = acc[:, :LANES] / acc[:, LANES:]
            mixed = gates_ref[0, p, b] * summary + gates_ref[1, p, b] * chosen
            m2 = mixed * mixed
            hi = m2.astype(BF16)
            lo = (m2 - hi.astype(F32)).astype(BF16)
            mean = dot_n(hi, sq) + dot_n(lo, sq)
            r = mixed * lax.rsqrt(mean + EPS)
            for tt in range(4):
                j0 = (tt % 2) * 2
                x = r[j0 * QB:(j0 + 1) * QB]
                y = r[(j0 + 1) * QB:(j0 + 2) * QB]
                if tt < 2:
                    z = jnp.where(lane1 < DH, x, pltpu.roll(y, DH, 1))
                else:
                    z = jnp.where(lane1 < DH, pltpu.roll(x, DH, 1), y)
                t = 4 * p + tt
                z = z * gain_ref[:, t * LANES:(t + 1) * LANES]
                out_ref[b * QB:(b + 1) * QB, t * LANES:(t + 1) * LANES] = z.astype(BF16)


def table_of(lists, my, n):
    groups = lists.shape[1]
    per = 256 // SLC
    sel = jnp.any(lists[:, :, None, :] == jnp.arange(n * per)[None, None, :, None], -1)
    sel = sel.reshape(2, groups, n, per).transpose(0, 2, 1, 3)
    own = lax.dynamic_slice_in_dim(sel, my, 1, 1)[:, 0].astype(jnp.int32)
    union = sel[0] | sel[1]
    u = union.astype(jnp.int32)
    before = jnp.stack([sum((u[..., i] for i in range(j)), jnp.zeros_like(u[..., 0])) for j in range(per)], -1)
    cols = []
    hits = [union & (before == slot) for slot in range(2)]
    for slot in range(2):
        cols.append(jnp.sum(jnp.where(hits[slot], jnp.arange(per), 0), -1))
    for b in range(2):
        for slot in range(2):
            cols.append(jnp.any(hits[slot] & sel[b], -1).astype(jnp.int32))
    tab = jnp.stack(cols, -1).reshape(-1)
    return jnp.concatenate([my.reshape(1).astype(jnp.int32), own.reshape(-1), tab.astype(jnp.int32)])


VM = pl.BlockSpec(memory_space=pltpu.VMEM)
SM = pl.BlockSpec(memory_space=pltpu.SMEM)


def per_device(n, queries, keys, values, gate_logits, chosen, pool_k, pool_v, out_gain):
    queries, keys, values = queries[0], keys[0], values[0]
    logits, lists = gate_logits[0], chosen[0]
    length = queries.shape[0]
    groups = keys.shape[1] // DH
    my = lax.axis_index("kv")
    last = n // 2

    def fw(k):
        return [(i, i + 1) for i in range(k - 1, n - 1)]

    def bw(k):
        return [((c - k + 1) % n, (c - k) % n) for c in range(last)]

    piece = jnp.concatenate([keys, values], 1)
    half = length // 2

    def hop(x, route):
        return lax.ppermute(x, "kv", route)

    f, g = hop(piece, fw(1)), hop(piece, bw(1))

    freq = THETA ** (-2.0 * np.arange(DH // 2) / DH)
    freq = np.tile(freq, LANES // (DH // 2))
    ang_a = (np.arange(n) * length)[:, None] * freq[None, :]
    ang_b = np.arange(length)[:, None] * freq[None, :]
    trigs = [jnp.asarray(a, F32) for a in (np.cos(ang_a), np.sin(ang_a), np.cos(ang_b), np.sin(ang_b))]
    tab = table_of(lists, my, n)
    rows = 4 * QB
    count = n * 16
    qs = jax.ShapeDtypeStruct((2, 2, rows, LANES), BF16)
    accs = jax.ShapeDtypeStruct((2, 2, rows, 2 * LANES), F32)
    ms = jax.ShapeDtypeStruct((2, 2, 2, rows, LANES), F32)
    def lus(pieces):
        return jax.ShapeDtypeStruct((pieces, 2, 16, 2 * keys.shape[1]), F32)

    gs = jax.ShapeDtypeStruct((2, 2, 2, rows, LANES), F32)
    cost = pl.CostEstimate(flops=2_000_000_000, bytes_accessed=4_000_000, transcendentals=1_000_000)
    params = pltpu.CompilerParams(vmem_limit_bytes=20 * 1024 * 1024)
    hbm = pl.BlockSpec(memory_space=pltpu.HBM)
    tabs = [jax.ShapeDtypeStruct(t.shape, F32) for t in trigs]
    loads = [queries, keys, values, logits, pool_k, pool_v]
    qrot, qraw, gates, acc, m, lu, pool, *trigs = pl.pallas_call(
        prep_body, out_shape=(qs, qs, gs, accs, ms, lus(1), jax.ShapeDtypeStruct((CMP_BLOCK, 2 * keys.shape[1]), F32), *tabs),
        in_specs=[SM] + [hbm] * 10, out_specs=(VM,) * 11,
        scratch_shapes=[pltpu.VMEM(x.shape, x.dtype) for x in loads] + [pltpu.SemaphoreType.DMA((10,))],
        compiler_params=params, cost_estimate=cost, name="prep",
    )(tab, *loads, *trigs)

    parts = [lu]
    for k in range(1, last + 1):
        if k < last:
            f, g, acc = lax.optimization_barrier((f, g, acc))
        if k < last - 1:
            f2, g2 = hop(f, fw(k + 1)), hop(g, bw(k + 1))
        elif k == last - 1:
            f2, g2 = hop(f[:half], fw(k + 1)), hop(g[half:], bw(k + 1))
        if k < last:
            acc, m, lu = pl.pallas_call(
                functools.partial(pair_kernel, n), out_shape=(accs, ms, lus(2)),
                in_specs=[SM] * 2 + [VM] * 10, out_specs=(VM,) * 3,
                input_output_aliases={10: 0, 11: 1},
                scratch_shapes=[pltpu.VMEM((2, 512, LANES), BF16), pltpu.VMEM((2, 512, 2 * LANES), BF16)],
                compiler_params=params, cost_estimate=cost, name="pair",
            )(tab, jnp.full((1,), k, jnp.int32), f, g, pool, *trigs, qrot, acc, m)
            parts.append(lu)
            f, g = f2, g2
        else:
            out = pl.pallas_call(
                functools.partial(final_kernel, k, n),
                out_shape=jax.ShapeDtypeStruct(queries.shape, BF16),
                in_specs=[SM] + [VM] * (13 + len(parts)), out_specs=VM,
                scratch_shapes=[pltpu.VMEM(accs.shape, F32), pltpu.VMEM(ms.shape, F32), pltpu.VMEM((2, count + 16, 2 * keys.shape[1]), F32),
                                pltpu.VMEM((2, 256, LANES), BF16), pltpu.VMEM((2, 256, 2 * LANES), BF16),
                                pltpu.VMEM((length, 2 * keys.shape[1]), BF16), pltpu.VMEM(lus(1).shape, F32)],
                compiler_params=params, cost_estimate=cost, name="final",
            )(tab, f, g, pool, *trigs, qrot, acc, m, qraw, gates, out_gain.reshape(1, -1), *parts)
    return out[None]


def solution(mesh):
    in_specs = (
        P(("grp", "dp"), "kv", "tp"),
        P(("grp", "dp"), "kv", "tp"),
        P(("grp", "dp"), "kv", "tp"),
        P(("grp", "dp"), None, "kv", "tp"),
        P(("grp", "dp"), "kv", "tp", None),
        P(),
        P(),
        P("tp"),
    )
    out_specs = P(("grp", "dp"), "kv", "tp")
    return jax.shard_map(
        functools.partial(per_device, mesh.shape["kv"]), mesh=mesh, in_specs=in_specs, out_specs=out_specs, check_vma=False
    )
```

```python
import functools
import math

import jax
import jax.numpy as jnp
import numpy as np
from jax import lax
from jax.experimental import pallas as pl
from jax.experimental.pallas import tpu as pltpu
from jax.sharding import PartitionSpec as P

DH = 64
CMP_STRIDE = 16
CMP_BLOCK = 32
SLC = 64
QB = 128
NSEL = 16
THETA = 500000.0
EPS = 1e-06
NEG = -1e30
SCALE2 = DH ** (-0.5) * math.log2(math.e)
LANES = 128
F32 = jnp.float32
BF16 = jnp.bfloat16


def lane_of(rows):
    return lax.broadcasted_iota(jnp.int32, (rows, LANES), 1)


def swap_halves(x, lane):
    return jnp.where(lane % DH < DH // 2, pltpu.roll(x, 96, 1), pltpu.roll(x, 32, 1))


def trig(span, cosa, sina, cosb, sinb):
    ca = cosa[pl.ds(span, 1), :]
    sa = sina[pl.ds(span, 1), :]
    cos = ca * cosb - sa * sinb
    sin = sa * cosb + ca * sinb
    lane = lane_of(cosb.shape[0])
    return cos, jnp.where(lane % DH < DH // 2, -sin, sin)


def dot_t(a, b):
    return lax.dot_general(a, b, (((1,), (1,)), ((), ())), preferred_element_type=F32)


def dot_n(a, b):
    return lax.dot_general(a, b, (((1,), (0,)), ((), ())), preferred_element_type=F32)


def keep_half(x, odd):
    lane = lane_of(x.shape[0])
    return jnp.where((lane >= DH) if odd else (lane < DH), x, 0.0)


def with_ones(x, odd):
    ones = keep_half(jnp.ones((x.shape[0], LANES), F32), odd)
    return jnp.concatenate([keep_half(x, odd), ones], 1).astype(BF16)


def pools(piece, pool_ref, lu_ref, i):
    x = piece.astype(F32).reshape(16, CMP_STRIDE, -1)
    lower = jnp.sum(x * pool_ref[0:CMP_STRIDE, :][None], 1)
    upper = jnp.sum(x * pool_ref[CMP_STRIDE:CMP_BLOCK, :][None], 1)
    lu_ref[i, 0] = lower
    lu_ref[i, 1] = upper


def online(qrot_ref, rk, rv, bias_of, acc_in, m_in, acc_ref, m_ref, p):
    for b in range(2):
        s = dot_t(qrot_ref[p, b], rk) * SCALE2
        s = bias_of(b, s)
        n = s.shape[1] // LANES
        me = functools.reduce(jnp.maximum, [s[:, i * LANES:(i + 1) * LANES] for i in range(n) if bias_of.odd[i] == 0])
        mo = functools.reduce(jnp.maximum, [s[:, i * LANES:(i + 1) * LANES] for i in range(n) if bias_of.odd[i] == 1])
        rows = s.shape[0]
        me = jnp.broadcast_to(jnp.max(me, 1, keepdims=True), (rows, LANES))
        mo = jnp.broadcast_to(jnp.max(mo, 1, keepdims=True), (rows, LANES))
        if acc_in is not None:
            olde = m_in[p, b, 0]
            oldo = m_in[p, b, 1]
            me = jnp.maximum(me, olde)
            mo = jnp.maximum(mo, oldo)
            alpha = jnp.exp2(jnp.where(lane_of(rows) < DH, olde - me, oldo - mo))
        m_ref[p, b, 0] = me
        m_ref[p, b, 1] = mo
        w = jnp.concatenate(
            [jnp.exp2(s[:, i * LANES:(i + 1) * LANES] - (mo if bias_of.odd[i] else me)).astype(BF16) for i in range(n)], 1
        )
        out = dot_n(w, rv)
        if acc_in is not None:
            out = acc_in[p, b] * jnp.concatenate([alpha, alpha], 1) + out
        acc_ref[p, b] = out


class Bias:
    def __init__(self, odd, fn):
        self.odd = odd
        self.fn = fn

    def __call__(self, b, s):
        return self.fn(b, s)


def prep_body(tab, q_hbm, k_hbm, v_hbm, lg_hbm, pk_hbm, pv_hbm, cosa_hbm, sina_hbm, cosb_hbm, sinb_hbm,
              qrot_ref, qraw_ref, gates_ref, acc_ref, m_ref, lu_ref, pool_ref, cosa, sina, cosb_ref, sinb_ref,
              q_ref, k_ref, v_ref, lg_ref, pk_ref, pv_ref, sems):
    my = tab[0]
    moves = [pltpu.make_async_copy(src, dst, sems.at[i]) for i, (src, dst) in enumerate(
        [(q_hbm, q_ref), (k_hbm, k_ref), (v_hbm, v_ref), (lg_hbm, lg_ref), (pk_hbm, pk_ref), (pv_hbm, pv_ref),
         (cosa_hbm, cosa), (sina_hbm, sina), (cosb_hbm, cosb_ref), (sinb_hbm, sinb_ref)])]
    for move in moves:
        move.start()
    for move in moves:
        move.wait()
    for i, ref in enumerate((pk_ref, pv_ref)):
        two = jnp.concatenate([ref[...], ref[...]], 1)
        pool_ref[:, 2 * i * LANES:2 * (i + 1) * LANES] = jnp.concatenate([two, two], 1)
    length = q_ref.shape[0]
    cos, sin = trig(my, cosa, sina, cosb_ref[...], sinb_ref[...])
    lane = lane_of(length)
    lg = jax.nn.sigmoid(lg_ref[0]), jax.nn.sigmoid(lg_ref[1])
    for p in range(2):
        for j in range(4):
            tiles = []
            for odd in range(2):
                t = 4 * p + 2 * odd + j // 2
                x = q_ref[:, t * LANES:(t + 1) * LANES].astype(F32)
                turned = x * cos + swap_halves(x, lane) * sin
                if (j % 2) != odd:
                    x = pltpu.roll(x, DH, 1)
                    turned = pltpu.roll(turned, DH, 1)
                tiles.append((x, turned))
            raw = jnp.where(lane < DH, tiles[0][0], tiles[1][0]).astype(BF16)
            rot = jnp.where(lane < DH, tiles[0][1], tiles[1][1]).astype(BF16)
            he, ho = 8 * p + j, 8 * p + 4 + j
            gs = [jnp.where(lane < DH, lg[i][:, he:he + 1], lg[i][:, ho:ho + 1]) for i in range(2)]
            for b in range(2):
                rows = slice(b * QB, (b + 1) * QB)
                dst = slice(j * QB, (j + 1) * QB)
                qraw_ref[p, b, dst, :] = raw[rows]
                qrot_ref[p, b, dst, :] = rot[rows]
                gates_ref[0, p, b, dst, :] = gs[0][rows]
                gates_ref[1, p, b, dst, :] = gs[1][rows]
    both = jnp.concatenate([k_ref[...], v_ref[...]], 1)
    pools(both, pool_ref, lu_ref, 0)
    key_pos = lax.broadcasted_iota(jnp.int32, (QB, length), 1)
    row_pos = lax.broadcasted_iota(jnp.int32, (QB, length), 0)
    blk = lax.broadcasted_iota(jnp.int32, (1, length), 1) // SLC
    @pl.loop(0, 2)
    def _(p):
        at = pl.multiple_of(p * LANES, LANES)
        kx = k_ref[:, pl.ds(at, LANES)].astype(F32)
        kx = kx * cos + swap_halves(kx, lane) * sin
        vx = v_ref[:, pl.ds(at, LANES)].astype(F32)
        rk = jnp.concatenate([keep_half(kx, 0), keep_half(kx, 1)], 0).astype(BF16)
        rv = jnp.concatenate([with_ones(vx, 0), with_ones(vx, 1)], 0)

        def own_bias(b, s):
            cols = []
            for odd in range(2):
                row = jnp.zeros((1, length), jnp.int32)
                for i in range(4):
                    row = jnp.where(blk == i, tab[1 + (b * 4 + 2 * p + odd) * 4 + i], row)
                ok = (row > 0) & (key_pos <= row_pos + b * QB)
                cols.append(jnp.where(ok, 0.0, NEG))
            bias = jnp.concatenate(cols, 1)
            return s + jnp.concatenate([bias] * 4, 0)

        online(qrot_ref, rk, rv, Bias([0, 0, 1, 1], own_bias), None, None, acc_ref, m_ref, p)


OWN = 1 + 2 * 4 * 4


def step_body(spans, pieces, tab, pool_ref, cosa, sina, cosb_ref, sinb_ref, qrot_ref, acc_in, m_in, acc_ref, m_ref, lu_ref, rk_ref, rv_ref):
    for i, piece in enumerate(pieces):
        pools(piece[...], pool_ref, lu_ref, i)
    lane = lane_of(SLC)
    col = lax.broadcasted_iota(jnp.int32, (1, LANES), 1)

    @pl.loop(0, 2)
    def _(p):
        kat = pl.multiple_of(p * LANES, LANES)
        vat = pl.multiple_of((2 + p) * LANES, LANES)
        for i, (piece, span) in enumerate(zip(pieces, spans)):
            for odd in range(2):
                for slot in range(2):
                    base = OWN + (span * 4 + 2 * p + odd) * 6
                    at = pl.multiple_of(tab[base + slot] * SLC, SLC)
                    cos, sin = trig(span, cosa, sina, cosb_ref[pl.ds(at, SLC), :], sinb_ref[pl.ds(at, SLC), :])
                    kx = piece[pl.ds(at, SLC), pl.ds(kat, LANES)].astype(F32)
                    kx = kx * cos + swap_halves(kx, lane) * sin
                    vx = piece[pl.ds(at, SLC), pl.ds(vat, LANES)].astype(F32)
                    dst = slice(i * 256 + odd * 128 + slot * 64, i * 256 + odd * 128 + slot * 64 + 64)
                    rk_ref[p, dst, :] = keep_half(kx, odd).astype(BF16)
                    rv_ref[p, dst, :] = with_ones(vx, odd)

        def bias(b, s):
            cols = []
            for span in spans:
                for odd in range(2):
                    base = OWN + (span * 4 + 2 * p + odd) * 6 + 2 + b * 2
                    row = jnp.where(col < SLC, tab[base], tab[base + 1])
                    cols.append(jnp.where(row > 0, 0.0, NEG))
            return s + jnp.concatenate(cols, 1)

        online(qrot_ref, rk_ref[p, 0:256 * len(pieces)], rv_ref[p, 0:256 * len(pieces)], Bias([0, 1] * len(pieces), bias), acc_in, m_in, acc_ref, m_ref, p)


def pair_kernel(n, tab, step, p1_ref, p2_ref, pool_ref, cosa, sina, cosb_ref, sinb_ref, qrot_ref, acc_in, m_in,
                acc_ref, m_ref, lu_ref, rk_ref, rv_ref, piece_ref):
    my = tab[0]
    core = tab[OWN + n * 24]
    k = step[0]
    ahead = my - k
    behind = my + k - n
    both = behind >= 0
    one = (ahead >= 0) & (behind < 0)

    @pl.when(both)
    def _():
        first = jnp.where(core == 0, ahead, behind)
        step_body([first, ahead + behind - first], [p1_ref, p2_ref], tab, pool_ref, cosa, sina, cosb_ref, sinb_ref, qrot_ref,
                  acc_in, m_in, acc_ref, m_ref, lu_ref, rk_ref, rv_ref)

    @pl.when(one & (core == 0))
    def _():
        piece_ref[...] = p1_ref[...]

    @pl.when(one & (core != 0))
    def _():
        piece_ref[...] = p2_ref[...]

    @pl.when(one)
    def _():
        step_body([ahead], [piece_ref], tab, pool_ref, cosa, sina, cosb_ref, sinb_ref, qrot_ref,
                  acc_in, m_in, acc_ref, m_ref, lu_ref, rk_ref, rv_ref)
        lu_ref[1] = jnp.zeros(lu_ref.shape[1:], F32)

    @pl.when(ahead < 0)
    def _():
        acc_ref[...] = acc_in[...]
        m_ref[...] = m_in[...]
        lu_ref[...] = jnp.zeros(lu_ref.shape, F32)


def final_kernel(k, n, tab, pf_ref, pb_ref, pool_ref, cosa, sina, cosb_ref, sinb_ref, qrot_ref, acc_in, m_in,
                 qraw_ref, gates_ref, gain_ref, *rest):
    parts, (out_ref, acc_ref, m_ref, lu_ref, rk_ref, rv_ref, piece_ref, last_ref) = rest[:k], rest[k:]
    my = tab[0]
    half = pf_ref.shape[0]

    @pl.when(my >= k)
    def _():
        piece_ref[:half, :] = pf_ref[...]
        piece_ref[half:, :] = pb_ref[...]
        step_body([my - k], [piece_ref], tab, pool_ref, cosa, sina, cosb_ref, sinb_ref, qrot_ref,
                  acc_in, m_in, acc_ref, m_ref, last_ref, rk_ref, rv_ref)

    @pl.when(my < k)
    def _():
        acc_ref[...] = acc_in[...]
        last_ref[...] = jnp.zeros(last_ref.shape, F32)

    lu_ref[:, 16 * n:, :] = jnp.zeros((2, 16, lu_ref.shape[2]), F32)

    def place(part, i, span):
        at = pl.multiple_of(span * 16, 16)
        for half in range(2):
            lu_ref[half, pl.ds(at, 16), :] = part[i, half]

    place(parts[0], 0, my)
    core = tab[OWN + n * 24]
    for d in range(1, k):
        ahead = lax.rem(my + n - d, n)
        behind = lax.rem(my + d, n)
        swapped = (core != 0) & (my + d >= n)
        place(parts[d], 0, jnp.where(swapped, behind, ahead))
        place(parts[d], 1, jnp.where(swapped, ahead, behind))
    place(last_ref, 0, lax.rem(my + n - k, n))
    count = 16 * n
    sums = (lu_ref[0, 0:count, :] + lu_ref[1, 1:count + 1, :]).astype(BF16).astype(F32)
    length = 2 * QB
    ends = lax.broadcasted_iota(jnp.int32, (QB, count), 1) * CMP_STRIDE + CMP_BLOCK - 1
    row_pos = lax.broadcasted_iota(jnp.int32, (QB, count), 0)
    rows = 4 * QB
    lane = lane_of(rows)
    lane1 = lane_of(QB)
    sq = lax.broadcasted_iota(jnp.int32, (LANES, LANES), 0) // DH == lax.broadcasted_iota(jnp.int32, (LANES, LANES), 1) // DH
    sq = jnp.where(sq, 1.0 / DH, 0.0).astype(BF16)
    for p in range(2):
        ks = sums[:, p * LANES:(p + 1) * LANES]
        vs = sums[:, (2 + p) * LANES:(3 + p) * LANES]
        for b in range(2):
            ok = ends <= row_pos + (my * length + b * QB)
            ok = jnp.concatenate([ok] * 4, 0)
            out = None
            for odd in range(2):
                s = dot_t(qraw_ref[p, b], keep_half(ks, odd).astype(BF16)) * SCALE2
                s = jnp.where(ok, s, NEG)
                top = jnp.max(s, 1, keepdims=True)
                w = jnp.where(ok, jnp.exp2(s - top), 0.0).astype(BF16)
                o = dot_n(w, with_ones(vs, odd))
                out = o if out is None else out + o
            summary = out[:, :LANES] / jnp.maximum(out[:, LANES:], 1.0)
            acc = acc_ref[p, b]
            chosen = acc[:, :LANES] / acc[:, LANES:]
            mixed = gates_ref[0, p, b] * summary + gates_ref[1, p, b] * chosen
            m2 = mixed * mixed
            hi = m2.astype(BF16)
            lo = (m2 - hi.astype(F32)).astype(BF16)
            mean = dot_n(hi, sq) + dot_n(lo, sq)
            r = mixed * lax.rsqrt(mean + EPS)
            for tt in range(4):
                j0 = (tt % 2) * 2
                x = r[j0 * QB:(j0 + 1) * QB]
                y = r[(j0 + 1) * QB:(j0 + 2) * QB]
                if tt < 2:
                    z = jnp.where(lane1 < DH, x, pltpu.roll(y, DH, 1))
                else:
                    z = jnp.where(lane1 < DH, pltpu.roll(x, DH, 1), y)
                t = 4 * p + tt
                z = z * gain_ref[:, t * LANES:(t + 1) * LANES]
                out_ref[b * QB:(b + 1) * QB, t * LANES:(t + 1) * LANES] = z.astype(BF16)


def table_of(lists, my, n):
    groups = lists.shape[1]
    per = 256 // SLC
    sel = jnp.any(lists[:, :, None, :] == jnp.arange(n * per)[None, None, :, None], -1)
    sel = sel.reshape(2, groups, n, per).transpose(0, 2, 1, 3)
    own = lax.dynamic_slice_in_dim(sel, my, 1, 1)[:, 0].astype(jnp.int32)
    union = sel[0] | sel[1]
    u = union.astype(jnp.int32)
    before = jnp.stack([sum((u[..., i] for i in range(j)), jnp.zeros_like(u[..., 0])) for j in range(per)], -1)
    cols = []
    hits = [union & (before == slot) for slot in range(2)]
    for slot in range(2):
        cols.append(jnp.sum(jnp.where(hits[slot], jnp.arange(per), 0), -1))
    for b in range(2):
        for slot in range(2):
            cols.append(jnp.any(hits[slot] & sel[b], -1).astype(jnp.int32))
    tab = jnp.stack(cols, -1).reshape(-1)
    core = lax.axis_index("tp").reshape(1)
    return jnp.concatenate([my.reshape(1).astype(jnp.int32), own.reshape(-1), tab.astype(jnp.int32), core.astype(jnp.int32)])


VM = pl.BlockSpec(memory_space=pltpu.VMEM)
SM = pl.BlockSpec(memory_space=pltpu.SMEM)


def per_device(n, queries, keys, values, gate_logits, chosen, pool_k, pool_v, out_gain):
    queries, keys, values = queries[0], keys[0], values[0]
    logits, lists = gate_logits[0], chosen[0]
    length = queries.shape[0]
    groups = keys.shape[1] // DH
    my = lax.axis_index("kv")
    last = n // 2

    def fw(k):
        return [(i, i + 1) for i in range(k - 1, n - 1)]

    def bw(k):
        return [((c - k + 1) % n, (c - k) % n) for c in range(last)]

    piece = jnp.concatenate([keys, values], 1)
    half = length // 2

    def both_cores(first, second):
        return [(2 * i, 2 * j) for i, j in first] + [(2 * i + 1, 2 * j + 1) for i, j in second]

    def hop1(x, k):
        return lax.ppermute(x, ("kv", "tp"), both_cores(fw(k), bw(k)))

    def hop2(x, k):
        return lax.ppermute(x, ("kv", "tp"), both_cores(bw(k), fw(k)))

    f, g = hop1(piece, 1), hop2(piece, 1)

    freq = THETA ** (-2.0 * np.arange(DH // 2) / DH)
    freq = np.tile(freq, LANES // (DH // 2))
    ang_a = (np.arange(n) * length)[:, None] * freq[None, :]
    ang_b = np.arange(length)[:, None] * freq[None, :]
    trigs = [jnp.asarray(a, F32) for a in (np.cos(ang_a), np.sin(ang_a), np.cos(ang_b), np.sin(ang_b))]
    tab = table_of(lists, my, n)
    rows = 4 * QB
    count = n * 16
    qs = jax.ShapeDtypeStruct((2, 2, rows, LANES), BF16)
    accs = jax.ShapeDtypeStruct((2, 2, rows, 2 * LANES), F32)
    ms = jax.ShapeDtypeStruct((2, 2, 2, rows, LANES), F32)
    def lus(pieces):
        return jax.ShapeDtypeStruct((pieces, 2, 16, 2 * keys.shape[1]), F32)

    gs = jax.ShapeDtypeStruct((2, 2, 2, rows, LANES), F32)
    cost = pl.CostEstimate(flops=2_000_000_000, bytes_accessed=4_000_000, transcendentals=1_000_000)
    params = pltpu.CompilerParams(vmem_limit_bytes=20 * 1024 * 1024)
    hbm = pl.BlockSpec(memory_space=pltpu.HBM)
    tabs = [jax.ShapeDtypeStruct(t.shape, F32) for t in trigs]
    loads = [queries, keys, values, logits, pool_k, pool_v]
    pinned = [pltpu.with_memory_space_constraint(x, pltpu.HBM) for x in loads + trigs]
    qrot, qraw, gates, acc, m, lu, pool, *trigs = pl.pallas_call(
        prep_body, out_shape=(qs, qs, gs, accs, ms, lus(1), jax.ShapeDtypeStruct((CMP_BLOCK, 2 * keys.shape[1]), F32), *tabs),
        in_specs=[SM] + [hbm] * 10, out_specs=(VM,) * 11,
        scratch_shapes=[pltpu.VMEM(x.shape, x.dtype) for x in loads] + [pltpu.SemaphoreType.DMA((10,))],
        compiler_params=params, cost_estimate=cost, name="prep",
    )(tab, *pinned)

    parts = [lu]
    for k in range(1, last + 1):
        if k < last:
            f, acc = lax.optimization_barrier((f, acc))
        if k < last - 1:
            f2, g2 = hop1(f, k + 1), hop2(g, k + 1)
        elif k == last - 1:
            f2, g2 = hop1(f[:half], k + 1), hop2(g[half:], k + 1)
        if k < last:
            acc, m, lu = pl.pallas_call(
                functools.partial(pair_kernel, n), out_shape=(accs, ms, lus(2)),
                in_specs=[SM] * 2 + [VM] * 10, out_specs=(VM,) * 3,
                input_output_aliases={10: 0, 11: 1},
                scratch_shapes=[pltpu.VMEM((2, 512, LANES), BF16), pltpu.VMEM((2, 512, 2 * LANES), BF16), pltpu.VMEM(piece.shape, BF16)],
                compiler_params=params, cost_estimate=cost, name="pair",
            )(tab, jnp.full((1,), k, jnp.int32), f, g, pool, *trigs, qrot, acc, m)
            parts.append(lu)
            f, g = f2, g2
        else:
            out = pl.pallas_call(
                functools.partial(final_kernel, k, n),
                out_shape=jax.ShapeDtypeStruct(queries.shape, BF16),
                in_specs=[SM] + [VM] * (13 + len(parts)), out_specs=VM,
                scratch_shapes=[pltpu.VMEM(accs.shape, F32), pltpu.VMEM(ms.shape, F32), pltpu.VMEM((2, count + 16, 2 * keys.shape[1]), F32),
                                pltpu.VMEM((2, 256, LANES), BF16), pltpu.VMEM((2, 256, 2 * LANES), BF16),
                                pltpu.VMEM((length, 2 * keys.shape[1]), BF16), pltpu.VMEM(lus(1).shape, F32)],
                compiler_params=params, cost_estimate=cost, name="final",
            )(tab, f, g, pool, *trigs, qrot, acc, m, qraw, gates, out_gain.reshape(1, -1), *parts)
    return out[None]


def solution(mesh):
    in_specs = (
        P(("grp", "dp"), "kv", "tp"),
        P(("grp", "dp"), "kv", "tp"),
        P(("grp", "dp"), "kv", "tp"),
        P(("grp", "dp"), None, "kv", "tp"),
        P(("grp", "dp"), "kv", "tp", None),
        P(),
        P(),
        P("tp"),
    )
    out_specs = P(("grp", "dp"), "kv", "tp")
    return jax.shard_map(
        functools.partial(per_device, mesh.shape["kv"]), mesh=mesh, in_specs=in_specs, out_specs=out_specs, check_vma=False
    )
```

```python
import functools
import math

import jax
import jax.numpy as jnp
import numpy as np
from jax import lax
from jax.experimental import pallas as pl
from jax.experimental.pallas import tpu as pltpu
from jax.sharding import PartitionSpec as P

DH = 64
CMP_STRIDE = 16
CMP_BLOCK = 32
SLC = 64
QB = 128
NSEL = 16
THETA = 500000.0
EPS = 1e-06
NEG = -1e30
SCALE2 = DH ** (-0.5) * math.log2(math.e)
LANES = 128
F32 = jnp.float32
BF16 = jnp.bfloat16


def lane_of(rows):
    return lax.broadcasted_iota(jnp.int32, (rows, LANES), 1)


def swap_halves(x, lane):
    return jnp.where(lane % DH < DH // 2, pltpu.roll(x, 96, 1), pltpu.roll(x, 32, 1))


def trig(span, cosa, sina, cosb, sinb):
    ca = cosa[pl.ds(span, 1), :]
    sa = sina[pl.ds(span, 1), :]
    cos = ca * cosb - sa * sinb
    sin = sa * cosb + ca * sinb
    lane = lane_of(cosb.shape[0])
    return cos, jnp.where(lane % DH < DH // 2, -sin, sin)


def dot_t(a, b):
    return lax.dot_general(a, b, (((1,), (1,)), ((), ())), preferred_element_type=F32)


def dot_n(a, b):
    return lax.dot_general(a, b, (((1,), (0,)), ((), ())), preferred_element_type=F32)


def keep_half(x, odd):
    lane = lane_of(x.shape[0])
    return jnp.where((lane >= DH) if odd else (lane < DH), x, 0.0)


def with_ones(x, odd):
    ones = keep_half(jnp.ones((x.shape[0], LANES), F32), odd)
    return jnp.concatenate([keep_half(x, odd), ones], 1).astype(BF16)


def pools(piece_ref, pool_ref, lu_ref, i):
    @pl.loop(0, 2)
    def _(t):
        cols = pl.ds(pl.multiple_of(t * 256, 256), 256)
        x = piece_ref[:, cols].astype(F32).reshape(16, CMP_STRIDE, -1)
        lu_ref[i, 0, :, cols] = jnp.sum(x * pool_ref[0:CMP_STRIDE, cols][None], 1)
        lu_ref[i, 1, :, cols] = jnp.sum(x * pool_ref[CMP_STRIDE:CMP_BLOCK, cols][None], 1)


def online(qrot_ref, rk, rv, bias_of, acc_in, m_in, acc_ref, m_ref, p):
    for b in range(2):
        s = dot_t(qrot_ref[p, b], rk) * SCALE2
        s = bias_of(b, s)
        n = s.shape[1] // LANES
        me = functools.reduce(jnp.maximum, [s[:, i * LANES:(i + 1) * LANES] for i in range(n) if bias_of.odd[i] == 0])
        mo = functools.reduce(jnp.maximum, [s[:, i * LANES:(i + 1) * LANES] for i in range(n) if bias_of.odd[i] == 1])
        rows = s.shape[0]
        me = jnp.broadcast_to(jnp.max(me, 1, keepdims=True), (rows, LANES))
        mo = jnp.broadcast_to(jnp.max(mo, 1, keepdims=True), (rows, LANES))
        if acc_in is not None:
            olde = m_in[p, b, 0]
            oldo = m_in[p, b, 1]
            me = jnp.maximum(me, olde)
            mo = jnp.maximum(mo, oldo)
            alpha = jnp.exp2(jnp.where(lane_of(rows) < DH, olde - me, oldo - mo))
        m_ref[p, b, 0] = me
        m_ref[p, b, 1] = mo
        w = jnp.concatenate(
            [jnp.exp2(s[:, i * LANES:(i + 1) * LANES] - (mo if bias_of.odd[i] else me)).astype(BF16) for i in range(n)], 1
        )
        out = dot_n(w, rv)
        if acc_in is not None:
            out = acc_in[p, b] * jnp.concatenate([alpha, alpha], 1) + out
        acc_ref[p, b] = out


class Bias:
    def __init__(self, odd, fn):
        self.odd = odd
        self.fn = fn

    def __call__(self, b, s):
        return self.fn(b, s)


def prep_body(tab, q_hbm, k_hbm, v_hbm, lg_hbm, pk_hbm, pv_hbm, cosa_hbm, sina_hbm, cosb_hbm, sinb_hbm,
              qrot_ref, qraw_ref, gates_ref, acc_ref, m_ref, lu_ref, pool_ref, cosa, sina, cosb_ref, sinb_ref,
              q_ref, k_ref, v_ref, lg_ref, pk_ref, pv_ref, sems, piece_ref):
    my = tab[0]
    moves = [pltpu.make_async_copy(src, dst, sems.at[i]) for i, (src, dst) in enumerate(
        [(q_hbm, q_ref), (k_hbm, k_ref), (v_hbm, v_ref), (lg_hbm, lg_ref), (pk_hbm, pk_ref), (pv_hbm, pv_ref),
         (cosa_hbm, cosa), (sina_hbm, sina), (cosb_hbm, cosb_ref), (sinb_hbm, sinb_ref)])]
    for move in moves:
        move.start()
    for move in moves:
        move.wait()
    for i, ref in enumerate((pk_ref, pv_ref)):
        two = jnp.concatenate([ref[...], ref[...]], 1)
        pool_ref[:, 2 * i * LANES:2 * (i + 1) * LANES] = jnp.concatenate([two, two], 1)
    length = q_ref.shape[0]
    cos, sin = trig(my, cosa, sina, cosb_ref[...], sinb_ref[...])
    lane = lane_of(length)
    lg = jax.nn.sigmoid(lg_ref[0]), jax.nn.sigmoid(lg_ref[1])
    for p in range(2):
        for j in range(4):
            tiles = []
            for odd in range(2):
                t = 4 * p + 2 * odd + j // 2
                x = q_ref[:, t * LANES:(t + 1) * LANES].astype(F32)
                turned = x * cos + swap_halves(x, lane) * sin
                if (j % 2) != odd:
                    x = pltpu.roll(x, DH, 1)
                    turned = pltpu.roll(turned, DH, 1)
                tiles.append((x, turned))
            raw = jnp.where(lane < DH, tiles[0][0], tiles[1][0]).astype(BF16)
            rot = jnp.where(lane < DH, tiles[0][1], tiles[1][1]).astype(BF16)
            he, ho = 8 * p + j, 8 * p + 4 + j
            gs = [jnp.where(lane < DH, lg[i][:, he:he + 1], lg[i][:, ho:ho + 1]) for i in range(2)]
            for b in range(2):
                rows = slice(b * QB, (b + 1) * QB)
                dst = slice(j * QB, (j + 1) * QB)
                qraw_ref[p, b, dst, :] = raw[rows]
                qrot_ref[p, b, dst, :] = rot[rows]
                gates_ref[0, p, b, dst, :] = gs[0][rows]
                gates_ref[1, p, b, dst, :] = gs[1][rows]
    piece_ref[:, :2 * LANES] = k_ref[...]
    piece_ref[:, 2 * LANES:] = v_ref[...]
    pools(piece_ref, pool_ref, lu_ref, 0)
    key_pos = lax.broadcasted_iota(jnp.int32, (QB, length), 1)
    row_pos = lax.broadcasted_iota(jnp.int32, (QB, length), 0)
    blk = lax.broadcasted_iota(jnp.int32, (1, length), 1) // SLC
    @pl.loop(0, 2)
    def _(p):
        at = pl.multiple_of(p * LANES, LANES)
        kx = k_ref[:, pl.ds(at, LANES)].astype(F32)
        kx = kx * cos + swap_halves(kx, lane) * sin
        vx = v_ref[:, pl.ds(at, LANES)].astype(F32)
        rk = jnp.concatenate([keep_half(kx, 0), keep_half(kx, 1)], 0).astype(BF16)
        rv = jnp.concatenate([with_ones(vx, 0), with_ones(vx, 1)], 0)

        def own_bias(b, s):
            cols = []
            for odd in range(2):
                row = jnp.zeros((1, length), jnp.int32)
                for i in range(4):
                    row = jnp.where(blk == i, tab[1 + (b * 4 + 2 * p + odd) * 4 + i], row)
                ok = (row > 0) & (key_pos <= row_pos + b * QB)
                cols.append(jnp.where(ok, 0.0, NEG))
            bias = jnp.concatenate(cols, 1)
            return s + jnp.concatenate([bias] * 4, 0)

        online(qrot_ref, rk, rv, Bias([0, 0, 1, 1], own_bias), None, None, acc_ref, m_ref, p)


OWN = 1 + 2 * 4 * 4


def step_body(spans, pieces, tab, pool_ref, cosa, sina, cosb_ref, sinb_ref, qrot_ref, acc_in, m_in, acc_ref, m_ref, lu_ref, rk_ref, rv_ref):
    for i, piece in enumerate(pieces):
        pools(piece, pool_ref, lu_ref, i)
    lane = lane_of(SLC)
    col = lax.broadcasted_iota(jnp.int32, (1, LANES), 1)

    @pl.loop(0, 2)
    def _(p):
        kat = pl.multiple_of(p * LANES, LANES)
        vat = pl.multiple_of((2 + p) * LANES, LANES)
        for i, (piece, span) in enumerate(zip(pieces, spans)):
            for odd in range(2):
                for slot in range(2):
                    base = OWN + (span * 4 + 2 * p + odd) * 6
                    at = pl.multiple_of(tab[base + slot] * SLC, SLC)
                    cos, sin = trig(span, cosa, sina, cosb_ref[pl.ds(at, SLC), :], sinb_ref[pl.ds(at, SLC), :])
                    kx = piece[pl.ds(at, SLC), pl.ds(kat, LANES)].astype(F32)
                    kx = kx * cos + swap_halves(kx, lane) * sin
                    vx = piece[pl.ds(at, SLC), pl.ds(vat, LANES)].astype(F32)
                    dst = slice(i * 256 + odd * 128 + slot * 64, i * 256 + odd * 128 + slot * 64 + 64)
                    rk_ref[p, dst, :] = keep_half(kx, odd).astype(BF16)
                    rv_ref[p, dst, :] = with_ones(vx, odd)

        def bias(b, s):
            cols = []
            for span in spans:
                for odd in range(2):
                    base = OWN + (span * 4 + 2 * p + odd) * 6 + 2 + b * 2
                    row = jnp.where(col < SLC, tab[base], tab[base + 1])
                    cols.append(jnp.where(row > 0, 0.0, NEG))
            return s + jnp.concatenate(cols, 1)

        online(qrot_ref, rk_ref[p, 0:256 * len(pieces)], rv_ref[p, 0:256 * len(pieces)], Bias([0, 1] * len(pieces), bias), acc_in, m_in, acc_ref, m_ref, p)


def pair_kernel(n, tab, step, p1_ref, p2_ref, pool_ref, cosa, sina, cosb_ref, sinb_ref, qrot_ref, acc_in, m_in,
                acc_ref, m_ref, lu_ref, rk_ref, rv_ref, piece_ref):
    my = tab[0]
    core = tab[OWN + n * 24]
    k = step[0]
    ahead = my - k
    behind = my + k - (n - 1)
    both = behind >= 0
    one = (ahead >= 0) & (behind < 0)

    @pl.when(both)
    def _():
        first = jnp.where(core == 0, ahead, behind)
        step_body([first, ahead + behind - first], [p1_ref, p2_ref], tab, pool_ref, cosa, sina, cosb_ref, sinb_ref, qrot_ref,
                  acc_in, m_in, acc_ref, m_ref, lu_ref, rk_ref, rv_ref)

    @pl.when(one & (core == 0))
    def _():
        piece_ref[...] = p1_ref[...]

    @pl.when(one & (core != 0))
    def _():
        piece_ref[...] = p2_ref[...]

    @pl.when(one)
    def _():
        step_body([ahead], [piece_ref], tab, pool_ref, cosa, sina, cosb_ref, sinb_ref, qrot_ref,
                  acc_in, m_in, acc_ref, m_ref, lu_ref, rk_ref, rv_ref)
        lu_ref[1] = jnp.zeros(lu_ref.shape[1:], F32)

    @pl.when(ahead < 0)
    def _():
        acc_ref[...] = acc_in[...]
        m_ref[...] = m_in[...]
        lu_ref[...] = jnp.zeros(lu_ref.shape, F32)


def final_kernel(k, n, tab, p_ref, pool_ref, cosa, sina, cosb_ref, sinb_ref, qrot_ref, acc_in, m_in,
                 qraw_ref, gates_ref, gain_ref, *rest):
    parts, (out_ref, acc_ref, m_ref, lu_ref, rk_ref, rv_ref, last_ref) = rest[:k + 1], rest[k + 1:]
    my = tab[0]
    lu_ref[...] = jnp.zeros(lu_ref.shape, F32)

    def place(part, i, span):
        at = pl.multiple_of(span * 16, 16)
        for half in range(2):
            lu_ref[half, pl.ds(at, 16), :] = part[i, half]

    @pl.when(my == n - 1)
    def _():
        step_body([0], [p_ref], tab, pool_ref, cosa, sina, cosb_ref, sinb_ref, qrot_ref,
                  acc_in, m_in, acc_ref, m_ref, last_ref, rk_ref, rv_ref)
        place(last_ref, 0, 0)

    @pl.when(my < n - 1)
    def _():
        acc_ref[...] = acc_in[...]

    place(parts[0], 0, my)
    core = tab[OWN + n * 24]
    for d in range(1, k + 1):
        ahead = lax.rem(my + n - d, n)
        around = my + d - (n - 1) >= 0
        behind = jnp.where(around, my + d - (n - 1), my + d)
        swapped = (core != 0) & around
        place(parts[d], 0, jnp.where(swapped, behind, ahead))
        place(parts[d], 1, jnp.where(swapped, ahead, behind))
    count = 16 * n
    length = 2 * QB
    ends = lax.broadcasted_iota(jnp.int32, (QB, count), 1) * CMP_STRIDE + CMP_BLOCK - 1
    row_pos = lax.broadcasted_iota(jnp.int32, (QB, count), 0)
    rows = 4 * QB
    lane = lane_of(rows)
    lane1 = lane_of(QB)
    sq = lax.broadcasted_iota(jnp.int32, (LANES, LANES), 0) // DH == lax.broadcasted_iota(jnp.int32, (LANES, LANES), 1) // DH
    sq = jnp.where(sq, 1.0 / DH, 0.0).astype(BF16)

    def sums(at):
        cols = pl.ds(pl.multiple_of(at * LANES, LANES), LANES)
        return (lu_ref[0, 0:count, cols] + lu_ref[1, 1:count + 1, cols]).astype(BF16).astype(F32)

    @pl.loop(0, 2)
    def _(p):
        ks = sums(p)
        vs = sums(2 + p)
        for b in range(2):
            ok = ends <= row_pos + (my * length + b * QB)
            ok = jnp.concatenate([ok] * 4, 0)
            out = None
            for odd in range(2):
                s = dot_t(qraw_ref[p, b], keep_half(ks, odd).astype(BF16)) * SCALE2
                s = jnp.where(ok, s, NEG)
                top = jnp.max(s, 1, keepdims=True)
                w = jnp.where(ok, jnp.exp2(s - top), 0.0).astype(BF16)
                o = dot_n(w, with_ones(vs, odd))
                out = o if out is None else out + o
            summary = out[:, :LANES] / jnp.maximum(out[:, LANES:], 1.0)
            acc = acc_ref[p, b]
            chosen = acc[:, :LANES] / acc[:, LANES:]
            mixed = gates_ref[0, p, b] * summary + gates_ref[1, p, b] * chosen
            m2 = mixed * mixed
            hi = m2.astype(BF16)
            lo = (m2 - hi.astype(F32)).astype(BF16)
            mean = dot_n(hi, sq) + dot_n(lo, sq)
            r = mixed * lax.rsqrt(mean + EPS)
            for tt in range(4):
                j0 = (tt % 2) * 2
                x = r[j0 * QB:(j0 + 1) * QB]
                y = r[(j0 + 1) * QB:(j0 + 2) * QB]
                if tt < 2:
                    z = jnp.where(lane1 < DH, x, pltpu.roll(y, DH, 1))
                else:
                    z = jnp.where(lane1 < DH, pltpu.roll(x, DH, 1), y)
                t = 4 * p + tt
                cols = pl.ds(pl.multiple_of(t * LANES, LANES), LANES)
                z = z * gain_ref[:, cols]
                out_ref[b * QB:(b + 1) * QB, cols] = z.astype(BF16)


def table_of(lists, my, n):
    groups = lists.shape[1]
    per = 256 // SLC
    sel = jnp.any(lists[:, :, None, :] == jnp.arange(n * per)[None, None, :, None], -1)
    sel = sel.reshape(2, groups, n, per).transpose(0, 2, 1, 3)
    own = lax.dynamic_slice_in_dim(sel, my, 1, 1)[:, 0].astype(jnp.int32)
    union = sel[0] | sel[1]
    u = union.astype(jnp.int32)
    before = jnp.stack([sum((u[..., i] for i in range(j)), jnp.zeros_like(u[..., 0])) for j in range(per)], -1)
    cols = []
    hits = [union & (before == slot) for slot in range(2)]
    for slot in range(2):
        cols.append(jnp.sum(jnp.where(hits[slot], jnp.arange(per), 0), -1))
    for b in range(2):
        for slot in range(2):
            cols.append(jnp.any(hits[slot] & sel[b], -1).astype(jnp.int32))
    tab = jnp.stack(cols, -1).reshape(-1)
    core = lax.axis_index("tp").reshape(1)
    return jnp.concatenate([my.reshape(1).astype(jnp.int32), own.reshape(-1), tab.astype(jnp.int32), core.astype(jnp.int32)])


VM = pl.BlockSpec(memory_space=pltpu.VMEM)
SM = pl.BlockSpec(memory_space=pltpu.SMEM)


def per_device(n, queries, keys, values, gate_logits, chosen, pool_k, pool_v, out_gain):
    queries, keys, values = queries[0], keys[0], values[0]
    logits, lists = gate_logits[0], chosen[0]
    length = queries.shape[0]
    groups = keys.shape[1] // DH
    my = lax.axis_index("kv")
    piece = jnp.concatenate([keys, values], 1)
    last = n // 2 - 1
    half = n // 2

    def fw(k):
        return [(i, i + 1) for i in range(k - 1, n - 1)]

    def at(c, k):
        return c - k if k < max(c, 1) else n - 1 + c - k

    def bw(k):
        return [(at(c, k - 1) if k > 1 or c else 0, at(c, k)) for c in range(half)]

    def both_cores(first, second):
        return [(2 * i, 2 * j) for i, j in first] + [(2 * i + 1, 2 * j + 1) for i, j in second]

    def hop1(x, k):
        return lax.ppermute(x, ("kv", "tp"), both_cores(fw(k), bw(k)))

    def hop2(x, k):
        return lax.ppermute(x, ("kv", "tp"), both_cores(bw(k), fw(k)))

    f, g = hop1(piece, 1), hop2(piece, 1)
    farthest = lax.ppermute(piece, ("kv", "tp"), both_cores([(0, n - 1)], [(0, n - 1)]))

    freq = THETA ** (-2.0 * np.arange(DH // 2) / DH)
    freq = np.tile(freq, LANES // (DH // 2))
    ang_a = (np.arange(n) * length)[:, None] * freq[None, :]
    ang_b = np.arange(length)[:, None] * freq[None, :]
    trigs = [jnp.asarray(a, F32) for a in (np.cos(ang_a), np.sin(ang_a), np.cos(ang_b), np.sin(ang_b))]
    tab = table_of(lists, my, n)
    rows = 4 * QB
    count = n * 16
    qs = jax.ShapeDtypeStruct((2, 2, rows, LANES), BF16)
    accs = jax.ShapeDtypeStruct((2, 2, rows, 2 * LANES), F32)
    ms = jax.ShapeDtypeStruct((2, 2, 2, rows, LANES), F32)
    def lus(pieces):
        return jax.ShapeDtypeStruct((pieces, 2, 16, 2 * keys.shape[1]), F32)

    gs = jax.ShapeDtypeStruct((2, 2, 2, rows, LANES), F32)
    cost = pl.CostEstimate(flops=2_000_000_000, bytes_accessed=4_000_000, transcendentals=1_000_000)
    params = pltpu.CompilerParams(vmem_limit_bytes=20 * 1024 * 1024)
    hbm = pl.BlockSpec(memory_space=pltpu.HBM)
    tabs = [jax.ShapeDtypeStruct(t.shape, F32) for t in trigs]
    loads = [queries, keys, values, logits, pool_k, pool_v]
    pinned = [pltpu.with_memory_space_constraint(x, pltpu.HBM) for x in loads + trigs]
    qrot, qraw, gates, acc, m, lu, pool, *trigs = pl.pallas_call(
        prep_body, out_shape=(qs, qs, gs, accs, ms, lus(1), jax.ShapeDtypeStruct((CMP_BLOCK, 2 * keys.shape[1]), F32), *tabs),
        in_specs=[SM] + [hbm] * 10, out_specs=(VM,) * 11,
        scratch_shapes=[pltpu.VMEM(x.shape, x.dtype) for x in loads] + [pltpu.SemaphoreType.DMA((10,)), pltpu.VMEM(piece.shape, BF16)],
        compiler_params=params, cost_estimate=cost, name="prep",
    )(tab, *pinned)

    parts = [lu]
    for k in range(1, last + 1):
        if k < last:
            if k == 2:
                f, acc, farthest = lax.optimization_barrier((f, acc, farthest))
            else:
                f, acc = lax.optimization_barrier((f, acc))
            f2, g2 = hop1(f, k + 1), hop2(g, k + 1)
        acc, m, lu = pl.pallas_call(
            functools.partial(pair_kernel, n), out_shape=(accs, ms, lus(2)),
            in_specs=[SM] * 2 + [VM] * 10, out_specs=(VM,) * 3,
            input_output_aliases={10: 0, 11: 1},
            scratch_shapes=[pltpu.VMEM((2, 512, LANES), BF16), pltpu.VMEM((2, 512, 2 * LANES), BF16), pltpu.VMEM(piece.shape, BF16)],
            compiler_params=params, cost_estimate=cost, name="pair",
        )(tab, jnp.full((1,), k, jnp.int32), f, g, pool, *trigs, qrot, acc, m)
        parts.append(lu)
        if k < last:
            f, g = f2, g2
    out = pl.pallas_call(
        functools.partial(final_kernel, last, n),
        out_shape=jax.ShapeDtypeStruct(queries.shape, BF16),
        in_specs=[SM] + [VM] * (12 + len(parts)), out_specs=VM,
        scratch_shapes=[pltpu.VMEM(accs.shape, F32), pltpu.VMEM(ms.shape, F32), pltpu.VMEM((2, count + 16, 2 * keys.shape[1]), F32),
                        pltpu.VMEM((2, 256, LANES), BF16), pltpu.VMEM((2, 256, 2 * LANES), BF16),
                        pltpu.VMEM(lus(1).shape, F32)],
        compiler_params=params, cost_estimate=cost, name="final",
    )(tab, farthest, pool, *trigs, qrot, acc, m, qraw, gates, out_gain.reshape(1, -1), *parts)
    return out[None]


def solution(mesh):
    in_specs = (
        P(("grp", "dp"), "kv", "tp"),
        P(("grp", "dp"), "kv", "tp"),
        P(("grp", "dp"), "kv", "tp"),
        P(("grp", "dp"), None, "kv", "tp"),
        P(("grp", "dp"), "kv", "tp", None),
        P(),
        P(),
        P("tp"),
    )
    out_specs = P(("grp", "dp"), "kv", "tp")
    return jax.shard_map(
        functools.partial(per_device, mesh.shape["kv"]), mesh=mesh, in_specs=in_specs, out_specs=out_specs, check_vma=False
    )
```

```python
import functools
import math

import jax
import jax.numpy as jnp
import numpy as np
from jax import lax
from jax.experimental import pallas as pl
from jax.experimental.pallas import tpu as pltpu
from jax.sharding import PartitionSpec as P

DH = 64
CMP_STRIDE = 16
CMP_BLOCK = 32
SLC = 64
QB = 128
NSEL = 16
THETA = 500000.0
EPS = 1e-06
NEG = -1e30
SCALE2 = DH ** (-0.5) * math.log2(math.e)
LANES = 128
DIRECT = 2
F32 = jnp.float32
BF16 = jnp.bfloat16


def lane_of(rows):
    return lax.broadcasted_iota(jnp.int32, (rows, LANES), 1)


def swap_halves(x, lane):
    return jnp.where(lane % DH < DH // 2, pltpu.roll(x, 96, 1), pltpu.roll(x, 32, 1))


def trig(span, cosa, sina, cosb, sinb):
    ca = cosa[pl.ds(span, 1), :]
    sa = sina[pl.ds(span, 1), :]
    cos = ca * cosb - sa * sinb
    sin = sa * cosb + ca * sinb
    lane = lane_of(cosb.shape[0])
    return cos, jnp.where(lane % DH < DH // 2, -sin, sin)


def dot_t(a, b):
    return lax.dot_general(a, b, (((1,), (1,)), ((), ())), preferred_element_type=F32)


def dot_n(a, b):
    return lax.dot_general(a, b, (((1,), (0,)), ((), ())), preferred_element_type=F32)


def keep_half(x, odd):
    lane = lane_of(x.shape[0])
    return jnp.where((lane >= DH) if odd else (lane < DH), x, 0.0)


def with_ones(x, odd):
    ones = keep_half(jnp.ones((x.shape[0], LANES), F32), odd)
    return jnp.concatenate([keep_half(x, odd), ones], 1).astype(BF16)


def pools(piece_ref, pool_ref, lu_ref, i):
    @pl.loop(0, 2)
    def _(t):
        cols = pl.ds(pl.multiple_of(t * 256, 256), 256)
        x = piece_ref[:, cols].astype(F32).reshape(16, CMP_STRIDE, -1)
        lu_ref[i, 0, :, cols] = jnp.sum(x * pool_ref[0:CMP_STRIDE, cols][None], 1)
        lu_ref[i, 1, :, cols] = jnp.sum(x * pool_ref[CMP_STRIDE:CMP_BLOCK, cols][None], 1)


def online(qrot_ref, rk, rv, bias_of, acc_in, m_in, acc_ref, m_ref, p):
    for b in range(2):
        s = dot_t(qrot_ref[p, b], rk) * SCALE2
        s = bias_of(b, s)
        n = s.shape[1] // LANES
        me = functools.reduce(jnp.maximum, [s[:, i * LANES:(i + 1) * LANES] for i in range(n) if bias_of.odd[i] == 0])
        mo = functools.reduce(jnp.maximum, [s[:, i * LANES:(i + 1) * LANES] for i in range(n) if bias_of.odd[i] == 1])
        rows = s.shape[0]
        me = jnp.broadcast_to(jnp.max(me, 1, keepdims=True), (rows, LANES))
        mo = jnp.broadcast_to(jnp.max(mo, 1, keepdims=True), (rows, LANES))
        if acc_in is not None:
            olde = m_in[p, b, 0]
            oldo = m_in[p, b, 1]
            me = jnp.maximum(me, olde)
            mo = jnp.maximum(mo, oldo)
            alpha = jnp.exp2(jnp.where(lane_of(rows) < DH, olde - me, oldo - mo))
        m_ref[p, b, 0] = me
        m_ref[p, b, 1] = mo
        w = jnp.concatenate(
            [jnp.exp2(s[:, i * LANES:(i + 1) * LANES] - (mo if bias_of.odd[i] else me)).astype(BF16) for i in range(n)], 1
        )
        out = dot_n(w, rv)
        if acc_in is not None:
            out = acc_in[p, b] * jnp.concatenate([alpha, alpha], 1) + out
        acc_ref[p, b] = out


class Bias:
    def __init__(self, odd, fn):
        self.odd = odd
        self.fn = fn

    def __call__(self, b, s):
        return self.fn(b, s)


def prep_body(tab, q_hbm, k_hbm, v_hbm, lg_hbm, pk_hbm, pv_hbm, cosa_hbm, sina_hbm, cosb_hbm, sinb_hbm,
              qrot_ref, qraw_ref, gates_ref, acc_ref, m_ref, lu_ref, pool_ref, cosa, sina, cosb_ref, sinb_ref,
              q_ref, k_ref, v_ref, lg_ref, pk_ref, pv_ref, sems, piece_ref):
    my = tab[0]
    moves = [pltpu.make_async_copy(src, dst, sems.at[i]) for i, (src, dst) in enumerate(
        [(q_hbm, q_ref), (k_hbm, k_ref), (v_hbm, v_ref), (lg_hbm, lg_ref), (pk_hbm, pk_ref), (pv_hbm, pv_ref),
         (cosa_hbm, cosa), (sina_hbm, sina), (cosb_hbm, cosb_ref), (sinb_hbm, sinb_ref)])]
    for move in moves:
        move.start()
    for move in moves:
        move.wait()
    for i, ref in enumerate((pk_ref, pv_ref)):
        two = jnp.concatenate([ref[...], ref[...]], 1)
        pool_ref[:, 2 * i * LANES:2 * (i + 1) * LANES] = jnp.concatenate([two, two], 1)
    length = q_ref.shape[0]
    cos, sin = trig(my, cosa, sina, cosb_ref[...], sinb_ref[...])
    lane = lane_of(length)
    lg = jax.nn.sigmoid(lg_ref[0]), jax.nn.sigmoid(lg_ref[1])
    for p in range(2):
        for j in range(4):
            tiles = []
            for odd in range(2):
                t = 4 * p + 2 * odd + j // 2
                x = q_ref[:, t * LANES:(t + 1) * LANES].astype(F32)
                turned = x * cos + swap_halves(x, lane) * sin
                if (j % 2) != odd:
                    x = pltpu.roll(x, DH, 1)
                    turned = pltpu.roll(turned, DH, 1)
                tiles.append((x, turned))
            raw = jnp.where(lane < DH, tiles[0][0], tiles[1][0]).astype(BF16)
            rot = jnp.where(lane < DH, tiles[0][1], tiles[1][1]).astype(BF16)
            he, ho = 8 * p + j, 8 * p + 4 + j
            gs = [jnp.where(lane < DH, lg[i][:, he:he + 1], lg[i][:, ho:ho + 1]) for i in range(2)]
            for b in range(2):
                rows = slice(b * QB, (b + 1) * QB)
                dst = slice(j * QB, (j + 1) * QB)
                qraw_ref[p, b, dst, :] = raw[rows]
                qrot_ref[p, b, dst, :] = rot[rows]
                gates_ref[0, p, b, dst, :] = gs[0][rows]
                gates_ref[1, p, b, dst, :] = gs[1][rows]
    piece_ref[:, :2 * LANES] = k_ref[...]
    piece_ref[:, 2 * LANES:] = v_ref[...]
    pools(piece_ref, pool_ref, lu_ref, 0)
    key_pos = lax.broadcasted_iota(jnp.int32, (QB, length), 1)
    row_pos = lax.broadcasted_iota(jnp.int32, (QB, length), 0)
    blk = lax.broadcasted_iota(jnp.int32, (1, length), 1) // SLC
    @pl.loop(0, 2)
    def _(p):
        at = pl.multiple_of(p * LANES, LANES)
        kx = k_ref[:, pl.ds(at, LANES)].astype(F32)
        kx = kx * cos + swap_halves(kx, lane) * sin
        vx = v_ref[:, pl.ds(at, LANES)].astype(F32)
        rk = jnp.concatenate([keep_half(kx, 0), keep_half(kx, 1)], 0).astype(BF16)
        rv = jnp.concatenate([with_ones(vx, 0), with_ones(vx, 1)], 0)

        def own_bias(b, s):
            cols = []
            for odd in range(2):
                row = jnp.zeros((1, length), jnp.int32)
                for i in range(4):
                    row = jnp.where(blk == i, tab[1 + (b * 4 + 2 * p + odd) * 4 + i], row)
                ok = (row > 0) & (key_pos <= row_pos + b * QB)
                cols.append(jnp.where(ok, 0.0, NEG))
            bias = jnp.concatenate(cols, 1)
            return s + jnp.concatenate([bias] * 4, 0)

        online(qrot_ref, rk, rv, Bias([0, 0, 1, 1], own_bias), None, None, acc_ref, m_ref, p)


OWN = 1 + 2 * 4 * 4


def step_body(spans, pieces, tab, pool_ref, cosa, sina, cosb_ref, sinb_ref, qrot_ref, acc_in, m_in, acc_ref, m_ref, lu_ref, rk_ref, rv_ref):
    for i, piece in enumerate(pieces):
        pools(piece, pool_ref, lu_ref, i)
    lane = lane_of(SLC)
    col = lax.broadcasted_iota(jnp.int32, (1, LANES), 1)

    @pl.loop(0, 2)
    def _(p):
        kat = pl.multiple_of(p * LANES, LANES)
        vat = pl.multiple_of((2 + p) * LANES, LANES)
        for i, (piece, span) in enumerate(zip(pieces, spans)):
            for odd in range(2):
                for slot in range(2):
                    base = OWN + (span * 4 + 2 * p + odd) * 6
                    at = pl.multiple_of(tab[base + slot] * SLC, SLC)
                    cos, sin = trig(span, cosa, sina, cosb_ref[pl.ds(at, SLC), :], sinb_ref[pl.ds(at, SLC), :])
                    kx = piece[pl.ds(at, SLC), pl.ds(kat, LANES)].astype(F32)
                    kx = kx * cos + swap_halves(kx, lane) * sin
                    vx = piece[pl.ds(at, SLC), pl.ds(vat, LANES)].astype(F32)
                    dst = slice(i * 256 + odd * 128 + slot * 64, i * 256 + odd * 128 + slot * 64 + 64)
                    rk_ref[p, dst, :] = keep_half(kx, odd).astype(BF16)
                    rv_ref[p, dst, :] = with_ones(vx, odd)

        def bias(b, s):
            cols = []
            for span in spans:
                for odd in range(2):
                    base = OWN + (span * 4 + 2 * p + odd) * 6 + 2 + b * 2
                    row = jnp.where(col < SLC, tab[base], tab[base + 1])
                    cols.append(jnp.where(row > 0, 0.0, NEG))
            return s + jnp.concatenate(cols, 1)

        online(qrot_ref, rk_ref[p, 0:256 * len(pieces)], rv_ref[p, 0:256 * len(pieces)], Bias([0, 1] * len(pieces), bias), acc_in, m_in, acc_ref, m_ref, p)


def pair_kernel(n, tab, step, p1_ref, p2_ref, pool_ref, cosa, sina, cosb_ref, sinb_ref, qrot_ref, acc_in, m_in,
                acc_ref, m_ref, lu_ref, rk_ref, rv_ref, piece_ref):
    my = tab[0]
    core = tab[OWN + n * 24]
    k = step[0]
    ahead = my - k
    behind = my + k - (n - 1)
    both = behind >= 0
    one = (ahead >= 0) & (behind < 0)

    @pl.when(both)
    def _():
        first = jnp.where(core == 0, ahead, behind)
        step_body([first, ahead + behind - first], [p1_ref, p2_ref], tab, pool_ref, cosa, sina, cosb_ref, sinb_ref, qrot_ref,
                  acc_in, m_in, acc_ref, m_ref, lu_ref, rk_ref, rv_ref)

    @pl.when(one & (core == 0))
    def _():
        piece_ref[...] = p1_ref[...]

    @pl.when(one & (core != 0))
    def _():
        piece_ref[...] = p2_ref[...]

    @pl.when(one)
    def _():
        step_body([ahead], [piece_ref], tab, pool_ref, cosa, sina, cosb_ref, sinb_ref, qrot_ref,
                  acc_in, m_in, acc_ref, m_ref, lu_ref, rk_ref, rv_ref)
        lu_ref[1] = jnp.zeros(lu_ref.shape[1:], F32)

    @pl.when(ahead < 0)
    def _():
        acc_ref[...] = acc_in[...]
        m_ref[...] = m_in[...]
        lu_ref[...] = jnp.zeros(lu_ref.shape, F32)


def final_kernel(k, n, tab, p_ref, pool_ref, cosa, sina, cosb_ref, sinb_ref, qrot_ref, acc_in, m_in,
                 qraw_ref, gates_ref, gain_ref, *rest):
    parts, (out_ref, acc_ref, m_ref, lu_ref, rk_ref, rv_ref, last_ref) = rest[:k + 1], rest[k + 1:]
    my = tab[0]
    lu_ref[...] = jnp.zeros(lu_ref.shape, F32)

    def place(part, i, span):
        at = pl.multiple_of(span * 16, 16)
        for half in range(2):
            lu_ref[half, pl.ds(at, 16), :] = part[i, half]

    @pl.when(my == n - 1)
    def _():
        step_body([0], [p_ref], tab, pool_ref, cosa, sina, cosb_ref, sinb_ref, qrot_ref,
                  acc_in, m_in, acc_ref, m_ref, last_ref, rk_ref, rv_ref)
        place(last_ref, 0, 0)

    @pl.when(my < n - 1)
    def _():
        acc_ref[...] = acc_in[...]

    place(parts[0], 0, my)
    core = tab[OWN + n * 24]
    for d in range(1, k + 1):
        ahead = lax.rem(my + n - d, n)
        around = my + d - (n - 1) >= 0
        behind = jnp.where(around, my + d - (n - 1), my + d)
        swapped = (core != 0) & around
        place(parts[d], 0, jnp.where(swapped, behind, ahead))
        place(parts[d], 1, jnp.where(swapped, ahead, behind))
    count = 16 * n
    length = 2 * QB
    ends = lax.broadcasted_iota(jnp.int32, (QB, count), 1) * CMP_STRIDE + CMP_BLOCK - 1
    row_pos = lax.broadcasted_iota(jnp.int32, (QB, count), 0)
    rows = 4 * QB
    lane = lane_of(rows)
    lane1 = lane_of(QB)
    sq = lax.broadcasted_iota(jnp.int32, (LANES, LANES), 0) // DH == lax.broadcasted_iota(jnp.int32, (LANES, LANES), 1) // DH
    sq = jnp.where(sq, 1.0 / DH, 0.0).astype(BF16)

    def sums(at):
        cols = pl.ds(pl.multiple_of(at * LANES, LANES), LANES)
        return (lu_ref[0, 0:count, cols] + lu_ref[1, 1:count + 1, cols]).astype(BF16).astype(F32)

    @pl.loop(0, 2)
    def _(p):
        ks = sums(p)
        vs = sums(2 + p)
        for b in range(2):
            ok = ends <= row_pos + (my * length + b * QB)
            ok = jnp.concatenate([ok] * 4, 0)
            out = None
            for odd in range(2):
                s = dot_t(qraw_ref[p, b], keep_half(ks, odd).astype(BF16)) * SCALE2
                s = jnp.where(ok, s, NEG)
                top = jnp.max(s, 1, keepdims=True)
                w = jnp.where(ok, jnp.exp2(s - top), 0.0).astype(BF16)
                o = dot_n(w, with_ones(vs, odd))
                out = o if out is None else out + o
            summary = out[:, :LANES] / jnp.maximum(out[:, LANES:], 1.0)
            acc = acc_ref[p, b]
            chosen = acc[:, :LANES] / acc[:, LANES:]
            mixed = gates_ref[0, p, b] * summary + gates_ref[1, p, b] * chosen
            m2 = mixed * mixed
            hi = m2.astype(BF16)
            lo = (m2 - hi.astype(F32)).astype(BF16)
            mean = dot_n(hi, sq) + dot_n(lo, sq)
            r = mixed * lax.rsqrt(mean + EPS)
            for tt in range(4):
                j0 = (tt % 2) * 2
                x = r[j0 * QB:(j0 + 1) * QB]
                y = r[(j0 + 1) * QB:(j0 + 2) * QB]
                if tt < 2:
                    z = jnp.where(lane1 < DH, x, pltpu.roll(y, DH, 1))
                else:
                    z = jnp.where(lane1 < DH, pltpu.roll(x, DH, 1), y)
                t = 4 * p + tt
                cols = pl.ds(pl.multiple_of(t * LANES, LANES), LANES)
                z = z * gain_ref[:, cols]
                out_ref[b * QB:(b + 1) * QB, cols] = z.astype(BF16)


def table_of(lists, my, n):
    groups = lists.shape[1]
    per = 256 // SLC
    sel = jnp.any(lists[:, :, None, :] == jnp.arange(n * per)[None, None, :, None], -1)
    sel = sel.reshape(2, groups, n, per).transpose(0, 2, 1, 3)
    own = lax.dynamic_slice_in_dim(sel, my, 1, 1)[:, 0].astype(jnp.int32)
    union = sel[0] | sel[1]
    u = union.astype(jnp.int32)
    before = jnp.stack([sum((u[..., i] for i in range(j)), jnp.zeros_like(u[..., 0])) for j in range(per)], -1)
    cols = []
    hits = [union & (before == slot) for slot in range(2)]
    for slot in range(2):
        cols.append(jnp.sum(jnp.where(hits[slot], jnp.arange(per), 0), -1))
    for b in range(2):
        for slot in range(2):
            cols.append(jnp.any(hits[slot] & sel[b], -1).astype(jnp.int32))
    tab = jnp.stack(cols, -1).reshape(-1)
    core = lax.axis_index("tp").reshape(1)
    return jnp.concatenate([my.reshape(1).astype(jnp.int32), own.reshape(-1), tab.astype(jnp.int32), core.astype(jnp.int32)])


VM = pl.BlockSpec(memory_space=pltpu.VMEM)
SM = pl.BlockSpec(memory_space=pltpu.SMEM)


def per_device(n, queries, keys, values, gate_logits, chosen, pool_k, pool_v, out_gain):
    queries, keys, values = queries[0], keys[0], values[0]
    logits, lists = gate_logits[0], chosen[0]
    length = queries.shape[0]
    groups = keys.shape[1] // DH
    my = lax.axis_index("kv")
    piece = jnp.concatenate([keys, values], 1)
    last = n // 2 - 1
    half = n // 2

    def fw(k):
        return [(i, i + 1) for i in range(k - 1, n - 1)]

    def at(c, k):
        if k < max(c, 1):
            return c if c >= half - DIRECT else c - k
        return n - 1 + c - k

    def bw(k):
        return [(at(c, k - 1), at(c, k)) for c in range(half)]

    def both_cores(first, second):
        return [(2 * i, 2 * j) for i, j in first] + [(2 * i + 1, 2 * j + 1) for i, j in second]

    def hop1(x, k):
        return lax.ppermute(x, ("kv", "tp"), both_cores(fw(k), bw(k)))

    def hop2(x, k):
        return lax.ppermute(x, ("kv", "tp"), both_cores(bw(k), fw(k)))

    f, g = hop1(piece, 1), hop2(piece, 1)
    farthest = lax.ppermute(piece, ("kv", "tp"), both_cores([(0, n - 1)], [(0, n - 1)]))

    freq = THETA ** (-2.0 * np.arange(DH // 2) / DH)
    freq = np.tile(freq, LANES // (DH // 2))
    ang_a = (np.arange(n) * length)[:, None] * freq[None, :]
    ang_b = np.arange(length)[:, None] * freq[None, :]
    trigs = [jnp.asarray(a, F32) for a in (np.cos(ang_a), np.sin(ang_a), np.cos(ang_b), np.sin(ang_b))]
    tab = table_of(lists, my, n)
    rows = 4 * QB
    count = n * 16
    qs = jax.ShapeDtypeStruct((2, 2, rows, LANES), BF16)
    accs = jax.ShapeDtypeStruct((2, 2, rows, 2 * LANES), F32)
    ms = jax.ShapeDtypeStruct((2, 2, 2, rows, LANES), F32)
    def lus(pieces):
        return jax.ShapeDtypeStruct((pieces, 2, 16, 2 * keys.shape[1]), F32)

    gs = jax.ShapeDtypeStruct((2, 2, 2, rows, LANES), F32)
    cost = pl.CostEstimate(flops=2_000_000_000, bytes_accessed=4_000_000, transcendentals=1_000_000)
    params = pltpu.CompilerParams(vmem_limit_bytes=20 * 1024 * 1024)
    hbm = pl.BlockSpec(memory_space=pltpu.HBM)
    tabs = [jax.ShapeDtypeStruct(t.shape, F32) for t in trigs]
    loads = [queries, keys, values, logits, pool_k, pool_v]
    pinned = [pltpu.with_memory_space_constraint(x, pltpu.HBM) for x in loads + trigs]
    qrot, qraw, gates, acc, m, lu, pool, *trigs = pl.pallas_call(
        prep_body, out_shape=(qs, qs, gs, accs, ms, lus(1), jax.ShapeDtypeStruct((CMP_BLOCK, 2 * keys.shape[1]), F32), *tabs),
        in_specs=[SM] + [hbm] * 10, out_specs=(VM,) * 11,
        scratch_shapes=[pltpu.VMEM(x.shape, x.dtype) for x in loads] + [pltpu.SemaphoreType.DMA((10,)), pltpu.VMEM(piece.shape, BF16)],
        compiler_params=params, cost_estimate=cost, name="prep",
    )(tab, *pinned)

    parts = [lu]
    for k in range(1, last + 1):
        if k < last:
            if k == 2:
                f, acc, farthest = lax.optimization_barrier((f, acc, farthest))
            else:
                f, acc = lax.optimization_barrier((f, acc))
            f2, g2 = hop1(f, k + 1), hop2(g, k + 1)
        acc, m, lu = pl.pallas_call(
            functools.partial(pair_kernel, n), out_shape=(accs, ms, lus(2)),
            in_specs=[SM] * 2 + [VM] * 10, out_specs=(VM,) * 3,
            input_output_aliases={10: 0, 11: 1},
            scratch_shapes=[pltpu.VMEM((2, 512, LANES), BF16), pltpu.VMEM((2, 512, 2 * LANES), BF16), pltpu.VMEM(piece.shape, BF16)],
            compiler_params=params, cost_estimate=cost, name="pair",
        )(tab, jnp.full((1,), k, jnp.int32), f, g, pool, *trigs, qrot, acc, m)
        parts.append(lu)
        if k < last:
            f, g = f2, g2
    out = pl.pallas_call(
        functools.partial(final_kernel, last, n),
        out_shape=jax.ShapeDtypeStruct(queries.shape, BF16),
        in_specs=[SM] + [VM] * (12 + len(parts)), out_specs=VM,
        scratch_shapes=[pltpu.VMEM(accs.shape, F32), pltpu.VMEM(ms.shape, F32), pltpu.VMEM((2, count + 16, 2 * keys.shape[1]), F32),
                        pltpu.VMEM((2, 256, LANES), BF16), pltpu.VMEM((2, 256, 2 * LANES), BF16),
                        pltpu.VMEM(lus(1).shape, F32)],
        compiler_params=params, cost_estimate=cost, name="final",
    )(tab, farthest, pool, *trigs, qrot, acc, m, qraw, gates, out_gain.reshape(1, -1), *parts)
    return out[None]


def solution(mesh):
    in_specs = (
        P(("grp", "dp"), "kv", "tp"),
        P(("grp", "dp"), "kv", "tp"),
        P(("grp", "dp"), "kv", "tp"),
        P(("grp", "dp"), None, "kv", "tp"),
        P(("grp", "dp"), "kv", "tp", None),
        P(),
        P(),
        P("tp"),
    )
    out_specs = P(("grp", "dp"), "kv", "tp")
    return jax.shard_map(
        functools.partial(per_device, mesh.shape["kv"]), mesh=mesh, in_specs=in_specs, out_specs=out_specs, check_vma=False
    )
```
